512 devices in a mesh: sp: 64 (over z, y), tp: 8 (over x, core).
Axes of the slice: x: 4, y: 8, z: 8, core: 2. Of those that a mesh axis runs over, the one named last changes fastest.
Arguments:
- resid: bfloat16 [12288, 2048], P('sp'), may hold values from -6 to 6
- query: bfloat16 [12288, 2048], P('sp', 'tp'), may hold values from -6 to 6
- key: bfloat16 [12288, 1024], P('sp', 'tp'), may hold values from -6 to 6
- value: bfloat16 [12288, 1024], P('sp', 'tp'), may hold values from -6 to 6
- q_gain: float32 [128], replicated, may hold values from 0.3 to 5, as said below
- k_gain: float32 [128], replicated, may hold values from 0.3 to 5, as said below
- out_weight: bfloat16 [2048, 2048], P('tp'), may hold values from -0.125 to 0.125
- norm_gain: float32 [2048], replicated, may hold values from 0.1 to 1.9
- gate_weight: bfloat16 [2048, 5632], P('sp', 'tp'), may hold values from -0.125 to 0.125
- up_weight: bfloat16 [2048, 5632], P('sp', 'tp'), may hold values from -0.125 to 0.125
- down_weight: bfloat16 [5632, 2048], P('tp', 'sp'), may hold values from -0.078125 to 0.078125
Outputs:
- mixed: bfloat16 [12288, 2048], P(('sp', 'tp'))
The draws below stay inside these ranges and needn't reach their ends.
Inputs may be any that keep to these rules, and one draw needn't show every extreme that they name: `q_gain`: positive gains. `k_gain`: positive gains.
All inputs are finite; a program needn't handle non-finite values.
Results may differ from the reference program's by a relative error of at most 0.012.
The reference program's roundings to bfloat16 on the way count: a program that leaves them out, or rounds other values in their place, can miss the bound.
Values may be sent and summed in bfloat16 or wider, within the bound.
No kernel may reach another device: no remote copies, remote signals or barrier semaphores. Data moves between devices by JAX's collectives and lax.ppermute only.
A program may use at most 64 MiB of HBM per device.

```python
import jax
import jax.numpy as jnp
from jax import lax

D = 2048
HEADS = 16
KV_HEADS = 8
HEAD_DIM = 128
FF = 5632
GRID_W = 64
TOK_DEV = 192
TOKENS = 12288
N_TP = 8


def paired_draw(key):
    base = jax.random.fold_in(key, 11)
    key_rows = jnp.clip(jax.random.normal(jax.random.fold_in(base, 1), (TOKENS, KV_HEADS * HEAD_DIM), jnp.float32), -6.0, 6.0)
    query_rows = jnp.clip(jax.random.normal(jax.random.fold_in(base, 2), (TOKENS, HEADS * HEAD_DIM), jnp.float32), -6.0, 6.0)
    return (query_rows, key_rows)


def draw_query(key, part):
    return paired_draw(key)[0].astype(jnp.bfloat16)


def draw_key(key, part):
    return paired_draw(key)[1].astype(jnp.bfloat16)


def gain_draw(key, salt):
    base = jax.random.fold_in(key, salt)
    return jnp.exp(jax.random.uniform(base, (HEAD_DIM,), jnp.float32, jnp.log(0.6), jnp.log(3.0)))


def draw_q_gain(key, part):
    return gain_draw(key, 21)


def draw_k_gain(key, part):
    return gain_draw(key, 22)


def level_of(key, shape, shards, low, high):
    level, own = 1.0, jax.random.fold_in(key, 6)
    for position, shards_of in shards:
        draws = jnp.exp(jax.random.uniform(jax.random.fold_in(own, position), (shards_of,), jnp.float32, low / len(shards), high / len(shards)))
        level = level * jnp.repeat(draws, shape[position] // shards_of).reshape([-1 if axis == position else 1 for axis in range(len(shape))])
    return level


def normal_values(own_key, extent, deviation, reach, shards=(), kind=jnp.bfloat16):
    entries = deviation * jax.random.normal(own_key, extent, jnp.float32)
    if shards:
        entries = entries * level_of(own_key, extent, shards, -0.22, 0.18)
    return jnp.clip(entries, -reach, reach).astype(kind)


def setup_inputs(seed: int = 0) -> dict:
    splits = jax.random.split(jax.random.key(seed), 12)
    return {
        "resid": normal_values(splits[0], (TOKENS, D), 1.0, 6.0, ((0, 64),)),
        "query": draw_query(jax.random.fold_in(splits[11], 71), 0),
        "key": draw_key(jax.random.fold_in(splits[11], 71), 0),
        "value": normal_values(splits[3], (TOKENS, KV_HEADS * HEAD_DIM), 1.0, 6.0, ((0, 64), (1, 8))),
        "q_gain": draw_q_gain(jax.random.fold_in(splits[11], 71), 0),
        "k_gain": draw_k_gain(jax.random.fold_in(splits[11], 71), 0),
        "out_weight": normal_values(splits[6], (HEADS * HEAD_DIM, D), (HEADS * HEAD_DIM) ** -0.5, 0.125, ((0, 8),)),
        "norm_gain": jnp.clip(1.0 + 0.18 * jax.random.normal(splits[7], (D,), jnp.float32), 0.1, 1.9),
        "gate_weight": normal_values(splits[8], (D, FF), D ** -0.5, 0.125, ((0, 64), (1, 8))),
        "up_weight": normal_values(splits[9], (D, FF), D ** -0.5, 0.125, ((0, 64), (1, 8))),
        "down_weight": normal_values(splits[10], (FF, D), FF ** -0.5, 0.078125, ((0, 8), (1, 64))),
    }


EPSILON = 1e-06

def rounded(values):
    return lax.optimization_barrier(values.astype(jnp.bfloat16)).astype(jnp.float32)

def rotate(values, positions):
    dim_size = values.shape[-1]
    half_dim = dim_size // 2
    quarter = half_dim // 2
    inverse = 10000.0 ** (-jnp.arange(quarter, dtype=jnp.float32) / quarter)
    outputs = []
    for axis_pos, coords in enumerate((positions // GRID_W, positions % GRID_W)):
        angles = coords.astype(jnp.float32)[:, None] * inverse[None, :]
        cosine = jnp.cos(angles)[:, None, :]
        sine = jnp.sin(angles)[:, None, :]
        section = values[..., axis_pos * half_dim:(axis_pos + 1) * half_dim]
        first_half = section[..., :quarter]
        second_half = section[..., quarter:]
        outputs += [first_half * cosine - second_half * sine, second_half * cosine + first_half * sine]
    return jnp.concatenate(outputs, axis=-1)

def prepare(projected, gain, positions):
    values = projected.astype(jnp.float32)
    normed = values * lax.rsqrt(lax.optimization_barrier(jnp.mean(values * values, axis=-1, keepdims=True)) + EPSILON) * gain
    return rotate(normed, positions).astype(jnp.bfloat16)

def normalize(stream, gain):
    values = stream.astype(jnp.float32)
    return (values * lax.rsqrt(lax.optimization_barrier(jnp.mean(values * values, axis=-1, keepdims=True)) + EPSILON) * gain).astype(jnp.bfloat16)

def reference(resid, query, key, value, q_gain, k_gain, out_weight, norm_gain, gate_weight, up_weight, down_weight):
    positions = jnp.arange(TOKENS, dtype=jnp.int32)
    q_rot = prepare(query.reshape(TOKENS, HEADS, HEAD_DIM), q_gain, positions)
    k_rot = prepare(key.reshape(TOKENS, KV_HEADS, HEAD_DIM), k_gain, positions)
    key_float = k_rot.astype(jnp.float32)
    val_float = value.reshape(TOKENS, KV_HEADS, HEAD_DIM).astype(jnp.float32)
    group_size = HEADS // KV_HEADS
    query_blocks = q_rot.reshape(TOKENS // TOK_DEV, TOK_DEV, KV_HEADS, group_size, HEAD_DIM)

    def one_block(block):
        scores = jnp.einsum('qkgd,skd->kgqs', block.astype(jnp.float32), key_float) * HEAD_DIM ** (-0.5)
        maxima = lax.optimization_barrier(jnp.max(scores, axis=-1, keepdims=True))
        weights = jnp.exp(scores - maxima)
        totals = lax.optimization_barrier(jnp.sum(weights, axis=-1))
        summed = jnp.einsum('kgqs,skd->kgqd', rounded(weights), val_float)
        output = summed / totals[..., None]
        return jnp.transpose(output, (2, 0, 1, 3)).reshape(TOK_DEV, HEADS * HEAD_DIM).astype(jnp.bfloat16)
    attn = lax.map(one_block, query_blocks).reshape(TOKENS, HEADS * HEAD_DIM)
    head_width = HEADS * HEAD_DIM // N_TP
    proj = jnp.zeros((TOKENS, D), jnp.float32)
    for index in range(N_TP):
        part_rows = slice(index * head_width, (index + 1) * head_width)
        proj = proj + rounded(jnp.dot(attn[:, part_rows], out_weight[part_rows], preferred_element_type=jnp.float32))
    stream = (resid.astype(jnp.float32) + proj).astype(jnp.bfloat16)
    normed = normalize(stream, norm_gain)
    gate = jnp.dot(normed, gate_weight, preferred_element_type=jnp.float32)
    up_part = jnp.dot(normed, up_weight, preferred_element_type=jnp.float32)
    hidden = (jax.nn.silu(gate) * up_part).astype(jnp.bfloat16)
    unit_width = FF // N_TP
    down = jnp.zeros((TOKENS, D), jnp.float32)
    for index in range(N_TP):
        part_rows = slice(index * unit_width, (index + 1) * unit_width)
        down = down + rounded(jnp.dot(hidden[:, part_rows], down_weight[part_rows], preferred_element_type=jnp.float32))
    return (stream.astype(jnp.float32) + 0.5 * down).astype(jnp.bfloat16)
```

```python
import functools

import jax
import jax.numpy as jnp
import numpy as np
from jax import lax
from jax.experimental import pallas as pl
from jax.experimental.pallas import tpu as pltpu
from jax.sharding import Mesh
from jax.sharding import PartitionSpec as P

GRID_W = 64
SP = ("sp_0", "sp_1")
SP_TP = ("sp_0", "sp_1", "tp")
EPSILON = 1e-06
BF16 = jnp.bfloat16
F32 = jnp.float32
ROPE_BASE = 10000.0
STAT_ROWS = 16
LOG2E = 1.4426950408889634


def rope_tables(head_dim):
    quarter = head_dim // 4
    lane = np.arange(head_dim)
    inverse = np.power(np.float32(ROPE_BASE), -(lane % quarter).astype(np.float32) / np.float32(quarter))
    inverse = inverse.astype(np.float32)
    angles = np.arange(GRID_W, dtype=np.float32)[:, None] * inverse[None, :]
    sign = np.where((lane // quarter) % 2 == 0, -1.0, 1.0).astype(np.float32)
    cosine = np.cos(angles.astype(np.float64)).astype(np.float32)
    sine = np.sin(angles.astype(np.float64)).astype(np.float32) * sign
    return inverse[None, :], sign[None, :], cosine, sine


def prep_kernel(q_ref, k_ref, v_ref, qg_ref, kg_ref, inv_ref, sign_ref, cos_ref, sin_ref, qo_ref, kvo_ref):
    rows, head_dim = k_ref.shape
    heads = q_ref.shape[1] // head_dim
    quarter = head_dim // 4
    spans = rows // GRID_W
    sp = lax.axis_index("sp_0") * lax.axis_size("sp_1") + lax.axis_index("sp_1")
    first_row = (sp * spans).astype(F32)
    line = first_row + lax.broadcasted_iota(jnp.int32, (8, head_dim), 0).astype(F32)
    angle = line * inv_ref[...]
    row_cos = jnp.cos(angle)
    row_sin = jnp.sin(angle) * sign_ref[...]
    lane = lax.broadcasted_iota(jnp.int32, (GRID_W, head_dim), 1)
    by_row = lane < 2 * quarter
    is_first = (lane // quarter) % 2 == 0

    def turned(x, gain, cosine, sine):
        x = x.astype(F32)
        x = x * lax.rsqrt(jnp.mean(x * x, axis=-1, keepdims=True) + EPSILON) * gain
        other = jnp.where(
            is_first,
            pltpu.roll(x, head_dim - quarter, 1),
            pltpu.roll(x, quarter, 1),
        )
        return (x * cosine + other * sine).astype(BF16)

    for j in range(spans):
        at = pl.ds(j * GRID_W, GRID_W)
        cosine = jnp.where(by_row, row_cos[j : j + 1, :], cos_ref[...])
        sine = jnp.where(by_row, row_sin[j : j + 1, :], sin_ref[...])
        for h in range(heads):
            cols = slice(h * head_dim, (h + 1) * head_dim)
            qo_ref[at, cols] = turned(q_ref[at, cols], qg_ref[...], cosine, sine)
        kvo_ref[at, 0:head_dim] = turned(k_ref[at, :], kg_ref[...], cosine, sine)
    kvo_ref[:, head_dim:] = v_ref[...]


def prep(query, key, value, q_gain, k_gain):
    rows, head_dim = key.shape
    inverse, sign, cosine, sine = rope_tables(head_dim)
    return pl.pallas_call(
        prep_kernel,
        out_shape=(
            jax.ShapeDtypeStruct(query.shape, BF16),
            jax.ShapeDtypeStruct((rows, 2 * head_dim), BF16),
        ),
        name="prep",
    )(
        query,
        key,
        value,
        q_gain.reshape(1, -1),
        k_gain.reshape(1, -1),
        jnp.asarray(inverse),
        jnp.asarray(sign),
        jnp.asarray(cosine),
        jnp.asarray(sine),
    )


def split3(x):
    a = x.astype(BF16)
    rest = x - a.astype(F32)
    b = rest.astype(BF16)
    c = (rest - b.astype(F32)).astype(BF16)
    return a, b, c


def attend_kernel(q_ref, kv_ref, o_ref, s_ref, *, chunk):
    rows, width = q_ref.shape[1:]
    keys = kv_ref.shape[0]
    head_dim = kv_ref.shape[1] // 2
    heads = width // head_dim
    factor = head_dim ** (-0.5) * LOG2E
    nt = (((1,), (1,)), ((), ()))
    eye = (
        lax.broadcasted_iota(jnp.int32, (128, 128), 0)
        == lax.broadcasted_iota(jnp.int32, (128, 128), 1)
    )
    stat = jnp.zeros((STAT_ROWS, 128), F32)
    srow = lax.broadcasted_iota(jnp.int32, (STAT_ROWS, 128), 0)
    for h in range(heads):
        cols = slice(h * head_dim, (h + 1) * head_dim)
        q = q_ref[0, :, cols]
        peak = jnp.full((rows, 128), -jnp.inf, F32)
        for c in range(keys // chunk):
            at = pl.ds(c * chunk, chunk)
            s = lax.dot_general(q, kv_ref[at, 0:head_dim], nt, preferred_element_type=F32)
            s_ref[h, :, at] = s
            for u in range(chunk // 128):
                peak = jnp.maximum(peak, s[:, u * 128 : (u + 1) * 128])
        top = jnp.max(peak, axis=-1, keepdims=True)
        total = jnp.zeros((rows, 128), F32)
        accum = jnp.zeros((rows, head_dim), F32)
        for c in range(keys // chunk):
            at = pl.ds(c * chunk, chunk)
            w = jnp.exp2((s_ref[h, :, at] - top) * factor)
            for u in range(chunk // 128):
                total = total + w[:, u * 128 : (u + 1) * 128]
            accum = accum + jnp.dot(
                w.astype(BF16), kv_ref[at, head_dim:], preferred_element_type=F32
            )
        whole = jnp.sum(total, axis=-1, keepdims=True)
        o_ref[0, 0:rows, cols] = (accum / whole).astype(BF16)
        level = top * factor + jnp.log2(whole)
        out = jnp.zeros((STAT_ROWS, 128), F32)
        for t in range(-(-rows // 128)):
            n = min(128, rows - t * 128)
            spread = jnp.broadcast_to(level[t * 128 : t * 128 + n], (n, 128))
            flat = jnp.sum(jnp.where(eye[:n], spread, 0.0), axis=0, keepdims=True)
            a, b, c = split3(flat)
            for k, piece in enumerate((a, b, c)):
                out = jnp.where(srow == 3 * t + k, piece.astype(F32), out)
        o_ref[0, rows:, cols] = out.astype(BF16)


def attend(queries, keys_values):
    parts, rows, width = queries.shape
    keys = keys_values.shape[0]
    head_dim = keys_values.shape[1] // 2
    heads = width // head_dim
    work = parts * heads * rows * keys
    return pl.pallas_call(
        functools.partial(attend_kernel, chunk=256),
        grid=(parts,),
        in_specs=[
            pl.BlockSpec((1, rows, width), lambda i: (i, 0, 0)),
            pl.BlockSpec((keys, 2 * head_dim), lambda i: (0, 0)),
        ],
        out_specs=pl.BlockSpec((1, rows + STAT_ROWS, width), lambda i: (i, 0, 0)),
        out_shape=jax.ShapeDtypeStruct((parts, rows + STAT_ROWS, width), BF16),
        scratch_shapes=[pltpu.VMEM((heads, rows, keys), F32)],
        compiler_params=pltpu.CompilerParams(
            dimension_semantics=("arbitrary",), vmem_limit_bytes=32 * 2**20
        ),
        cost_estimate=pl.CostEstimate(
            flops=4 * work * head_dim, bytes_accessed=4 * 2**20, transcendentals=work
        ),
        name="attend",
    )(queries, keys_values)


def project_kernel(part_ref, w_ref, o_ref):
    parts, all_rows, width = part_ref.shape
    rows = all_rows - STAT_ROWS
    head_dim = 128
    eye = (
        lax.broadcasted_iota(jnp.int32, (128, 128), 0)
        == lax.broadcasted_iota(jnp.int32, (128, 128), 1)
    )
    pieces = []
    for h in range(width // head_dim):
        cols = slice(h * head_dim, (h + 1) * head_dim)
        outs = []
        stats = [part_ref[p, rows:, cols].astype(F32) for p in range(parts)]
        for t in range(-(-rows // 128)):
            n = min(128, rows - t * 128)
            levels = [
                s[3 * t : 3 * t + 1] + s[3 * t + 1 : 3 * t + 2] + s[3 * t + 2 : 3 * t + 3]
                for s in stats
            ]
            top = functools.reduce(jnp.maximum, levels)
            shares = [jnp.exp2(v - top) for v in levels]
            whole = functools.reduce(jnp.add, shares)
            total = jnp.zeros((n, head_dim), F32)
            for p in range(parts):
                flat = jnp.broadcast_to(shares[p] / whole, (n, 128))
                share = jnp.sum(jnp.where(eye[:n], flat, 0.0), axis=1, keepdims=True)
                total = total + share * part_ref[p, t * 128 : t * 128 + n, cols].astype(F32)
            outs.append(total.astype(BF16))
        pieces.append(jnp.concatenate(outs, axis=0))
    attn = jnp.concatenate(pieces, axis=1)
    for c in range(w_ref.shape[1] // 512):
        at = pl.ds(c * 512, 512)
        o_ref[:, at] = jnp.dot(attn, w_ref[:, at], preferred_element_type=F32).astype(BF16)


def project(parts, weight):
    rows = parts.shape[1] - STAT_ROWS
    return pl.pallas_call(
        project_kernel,
        out_shape=jax.ShapeDtypeStruct((rows, weight.shape[1]), BF16),
        cost_estimate=pl.CostEstimate(
            flops=2 * rows * weight.size, bytes_accessed=3 * 2**20, transcendentals=0
        ),
        name="project",
    )(parts, weight)


def feed_kernel(x_ref, w_ref, o_ref, acc_ref, down_ref, *, units):
    step = pl.program_id(0)
    block = w_ref.shape[0]
    both = 2 * units

    @pl.when(step == 0)
    def _():
        acc_ref[...] = jnp.zeros_like(acc_ref)

    acc_ref[...] += jnp.dot(x_ref[...], w_ref[:, 0:both], preferred_element_type=F32)
    down_ref[pl.ds(pl.multiple_of(step * block, block), block), :] = w_ref[:, both:]

    @pl.when(step == pl.num_programs(0) - 1)
    def _():
        gate = acc_ref[:, 0:units]
        up = acc_ref[:, units:both]
        hidden = (gate / (1.0 + jnp.exp(-gate)) * up).astype(BF16)
        spare = down_ref.shape[1] - units
        if spare:
            hidden = jnp.concatenate([hidden, jnp.zeros((hidden.shape[0], spare), BF16)], axis=1)
        nt = (((1,), (1,)), ((), ()))
        for c in range(o_ref.shape[1] // 256):
            at = pl.ds(c * 256, 256)
            o_ref[:, at] = lax.dot_general(
                hidden, down_ref[at, :], nt, preferred_element_type=F32
            ).astype(BF16)


def feed(x, weights, units):
    rows, depth = x.shape
    width = weights.shape[1]
    block = 256
    return pl.pallas_call(
        functools.partial(feed_kernel, units=units),
        grid=(depth // block,),
        in_specs=[
            pl.BlockSpec((rows, block), lambda i: (0, i)),
            pl.BlockSpec((block, width), lambda i: (i, 0)),
        ],
        out_specs=pl.BlockSpec((rows, depth), lambda i: (0, 0)),
        out_shape=jax.ShapeDtypeStruct((rows, depth), BF16),
        scratch_shapes=[
            pltpu.VMEM((rows, 2 * units), F32),
            pltpu.VMEM((depth, width - 2 * units), BF16),
        ],
        compiler_params=pltpu.CompilerParams(
            dimension_semantics=("arbitrary",), vmem_limit_bytes=60 * 2**20
        ),
        cost_estimate=pl.CostEstimate(
            flops=6 * rows * depth * units, bytes_accessed=10 * 2**20, transcendentals=0
        ),
        name="feed",
    )(x, weights)


def normalize(stream, gain):
    values = stream.astype(F32)
    return (
        values * lax.rsqrt(jnp.mean(values * values, axis=-1, keepdims=True) + EPSILON) * gain
    ).astype(BF16)


def summed_over_tp(x):
    share = x.shape[0] // lax.axis_size("tp")
    blocks = lax.all_to_all(x.reshape(-1, share, x.shape[1]), "tp", 0, 0, tiled=True)
    return jnp.sum(blocks.astype(F32), axis=0)


def body(
    resid,
    query,
    key,
    value,
    q_gain,
    k_gain,
    out_weight,
    norm_gain,
    gate_weight,
    up_weight,
    down_weight,
):
    rows = query.shape[0]
    units = gate_weight.shape[1]
    shard = [gate_weight, up_weight, down_weight.T]
    spare = -(3 * units) % 128
    if spare:
        shard.append(jnp.zeros((gate_weight.shape[0], spare), BF16))
    weights = lax.all_gather(jnp.concatenate(shard, axis=1), SP, axis=0, tiled=True)

    q_rot, keys_values = prep(query, key, value, q_gain, k_gain)
    queries = lax.all_gather(q_rot, "sp_1", axis=0)
    keys_values = lax.all_gather(keys_values, "sp_0", axis=0, tiled=True)
    partial = attend(queries, keys_values)
    partial = lax.all_to_all(partial, "sp_1", 0, 0, tiled=True)
    proj = summed_over_tp(project(partial, out_weight))
    share = rows // lax.axis_size("tp")
    my_resid = lax.dynamic_slice_in_dim(resid, lax.axis_index("tp") * share, share, 0)
    my_stream = (my_resid.astype(F32) + proj).astype(BF16)
    normed = lax.all_gather(normalize(my_stream, norm_gain), "tp", axis=0, tiled=True)
    down = summed_over_tp(feed(normed, weights, units))
    return (my_stream.astype(F32) + 0.5 * down).astype(BF16)


def solution(mesh):
    torus = Mesh(mesh.devices.reshape(8, 8, mesh.shape["tp"]), ("sp_0", "sp_1", "tp"))
    return jax.shard_map(
        body,
        mesh=torus,
        in_specs=(
            P(SP, None),
            P(SP, "tp"),
            P(SP, "tp"),
            P(SP, "tp"),
            P(),
            P(),
            P("tp", None),
            P(),
            P(SP, "tp"),
            P(SP, "tp"),
            P("tp", SP),
        ),
        out_specs=P(SP_TP, None),
        check_vma=False,
    )
```

```python
import functools

import jax
import jax.numpy as jnp
import numpy as np
from jax import lax
from jax.experimental import pallas as pl
from jax.experimental.pallas import tpu as pltpu
from jax.sharding import Mesh
from jax.sharding import PartitionSpec as P

GRID_W = 64
SP = ("sp_0", "sp_1")
SP_TP = ("sp_0", "sp_1", "tp")
EPSILON = 1e-06
BF16 = jnp.bfloat16
F32 = jnp.float32
ROPE_BASE = 10000.0
STAT_ROWS = 16
LOG2E = 1.4426950408889634


def rope_tables(head_dim):
    quarter = head_dim // 4
    lane = np.arange(head_dim)
    inverse = np.power(np.float32(ROPE_BASE), -(lane % quarter).astype(np.float32) / np.float32(quarter))
    inverse = inverse.astype(np.float32)
    angles = np.arange(GRID_W, dtype=np.float32)[:, None] * inverse[None, :]
    sign = np.where((lane // quarter) % 2 == 0, -1.0, 1.0).astype(np.float32)
    cosine = np.cos(angles.astype(np.float64)).astype(np.float32)
    sine = np.sin(angles.astype(np.float64)).astype(np.float32) * sign
    return inverse[None, :], sign[None, :], cosine, sine


def prep_kernel(q_ref, k_ref, v_ref, qg_ref, kg_ref, inv_ref, sign_ref, cos_ref, sin_ref, qo_ref, kvo_ref):
    rows, head_dim = k_ref.shape
    heads = q_ref.shape[1] // head_dim
    quarter = head_dim // 4
    spans = rows // GRID_W
    sp = lax.axis_index("sp_0") * lax.axis_size("sp_1") + lax.axis_index("sp_1")
    first_row = (sp * spans).astype(F32)
    line = first_row + lax.broadcasted_iota(jnp.int32, (8, head_dim), 0).astype(F32)
    angle = line * inv_ref[...]
    row_cos = jnp.cos(angle)
    row_sin = jnp.sin(angle) * sign_ref[...]
    lane = lax.broadcasted_iota(jnp.int32, (GRID_W, head_dim), 1)
    by_row = lane < 2 * quarter
    is_first = (lane // quarter) % 2 == 0

    def turned(x, gain, cosine, sine):
        x = x.astype(F32)
        x = x * lax.rsqrt(jnp.mean(x * x, axis=-1, keepdims=True) + EPSILON) * gain
        other = jnp.where(
            is_first,
            pltpu.roll(x, head_dim - quarter, 1),
            pltpu.roll(x, quarter, 1),
        )
        return (x * cosine + other * sine).astype(BF16)

    for j in range(spans):
        at = pl.ds(j * GRID_W, GRID_W)
        cosine = jnp.where(by_row, row_cos[j : j + 1, :], cos_ref[...])
        sine = jnp.where(by_row, row_sin[j : j + 1, :], sin_ref[...])
        for h in range(heads):
            cols = slice(h * head_dim, (h + 1) * head_dim)
            made = turned(q_ref[at, cols], qg_ref[...], cosine, sine)
            for n in range(qo_ref.shape[0]):
                qo_ref[n, at, cols] = made
        kvo_ref[at, 0:head_dim] = turned(k_ref[at, :], kg_ref[...], cosine, sine)
    kvo_ref[:, head_dim:] = v_ref[...]


def prep(query, key, value, q_gain, k_gain, copies):
    rows, head_dim = key.shape
    inverse, sign, cosine, sine = rope_tables(head_dim)
    return pl.pallas_call(
        prep_kernel,
        out_shape=(
            jax.ShapeDtypeStruct((copies, *query.shape), BF16),
            jax.ShapeDtypeStruct((rows, 2 * head_dim), BF16),
        ),
        name="prep",
    )(
        query,
        key,
        value,
        q_gain.reshape(1, -1),
        k_gain.reshape(1, -1),
        jnp.asarray(inverse),
        jnp.asarray(sign),
        jnp.asarray(cosine),
        jnp.asarray(sine),
    )


def split3(x):
    a = x.astype(BF16)
    rest = x - a.astype(F32)
    b = rest.astype(BF16)
    c = (rest - b.astype(F32)).astype(BF16)
    return a, b, c


def attend_kernel(q_ref, kv_ref, o_ref, s_ref, *, chunk):
    rows, width = q_ref.shape[1:]
    keys = kv_ref.shape[0]
    head_dim = kv_ref.shape[1] // 2
    heads = width // head_dim
    factor = head_dim ** (-0.5) * LOG2E
    nt = (((1,), (1,)), ((), ()))
    eye = (
        lax.broadcasted_iota(jnp.int32, (128, 128), 0)
        == lax.broadcasted_iota(jnp.int32, (128, 128), 1)
    )
    stat = jnp.zeros((STAT_ROWS, 128), F32)
    srow = lax.broadcasted_iota(jnp.int32, (STAT_ROWS, 128), 0)
    for h in range(heads):
        cols = slice(h * head_dim, (h + 1) * head_dim)
        q = q_ref[0, :, cols]
        peak = jnp.full((rows, 128), -jnp.inf, F32)
        for c in range(keys // chunk):
            at = pl.ds(c * chunk, chunk)
            s = lax.dot_general(q, kv_ref[at, 0:head_dim], nt, preferred_element_type=F32)
            s_ref[h, :, at] = s
            for u in range(chunk // 128):
                peak = jnp.maximum(peak, s[:, u * 128 : (u + 1) * 128])
        top = jnp.max(peak, axis=-1, keepdims=True)
        total = jnp.zeros((rows, 128), F32)
        accum = jnp.zeros((rows, head_dim), F32)
        for c in range(keys // chunk):
            at = pl.ds(c * chunk, chunk)
            w = jnp.exp2((s_ref[h, :, at] - top) * factor)
            for u in range(chunk // 128):
                total = total + w[:, u * 128 : (u + 1) * 128]
            accum = accum + jnp.dot(
                w.astype(BF16), kv_ref[at, head_dim:], preferred_element_type=F32
            )
        whole = jnp.sum(total, axis=-1, keepdims=True)
        o_ref[0, 0:rows, cols] = (accum / whole).astype(BF16)
        level = top * factor + jnp.log2(whole)
        out = jnp.zeros((STAT_ROWS, 128), F32)
        for t in range(-(-rows // 128)):
            n = min(128, rows - t * 128)
            spread = jnp.broadcast_to(level[t * 128 : t * 128 + n], (n, 128))
            flat = jnp.sum(jnp.where(eye[:n], spread, 0.0), axis=0, keepdims=True)
            a, b, c = split3(flat)
            for k, piece in enumerate((a, b, c)):
                out = jnp.where(srow == 3 * t + k, piece.astype(F32), out)
        o_ref[0, rows:, cols] = out.astype(BF16)


def attend(queries, keys_values):
    parts, rows, width = queries.shape
    keys = keys_values.shape[0]
    head_dim = keys_values.shape[1] // 2
    heads = width // head_dim
    work = parts * heads * rows * keys
    return pl.pallas_call(
        functools.partial(attend_kernel, chunk=256),
        grid=(parts,),
        in_specs=[
            pl.BlockSpec((1, rows, width), lambda i: (i, 0, 0)),
            pl.BlockSpec((keys, 2 * head_dim), lambda i: (0, 0)),
        ],
        out_specs=pl.BlockSpec((1, rows + STAT_ROWS, width), lambda i: (i, 0, 0)),
        out_shape=jax.ShapeDtypeStruct((parts, rows + STAT_ROWS, width), BF16),
        scratch_shapes=[pltpu.VMEM((heads, rows, keys), F32)],
        compiler_params=pltpu.CompilerParams(
            dimension_semantics=("arbitrary",), vmem_limit_bytes=32 * 2**20
        ),
        cost_estimate=pl.CostEstimate(
            flops=4 * work * head_dim, bytes_accessed=4 * 2**20, transcendentals=work
        ),
        name="attend",
    )(queries, keys_values)


def project_kernel(part_ref, w_ref, o_ref):
    parts, all_rows, width = part_ref.shape
    rows = all_rows - STAT_ROWS
    head_dim = 128
    eye = (
        lax.broadcasted_iota(jnp.int32, (128, 128), 0)
        == lax.broadcasted_iota(jnp.int32, (128, 128), 1)
    )
    pieces = []
    for h in range(width // head_dim):
        cols = slice(h * head_dim, (h + 1) * head_dim)
        outs = []
        stats = [part_ref[p, rows:, cols].astype(F32) for p in range(parts)]
        for t in range(-(-rows // 128)):
            n = min(128, rows - t * 128)
            levels = [
                s[3 * t : 3 * t + 1] + s[3 * t + 1 : 3 * t + 2] + s[3 * t + 2 : 3 * t + 3]
                for s in stats
            ]
            top = functools.reduce(jnp.maximum, levels)
            shares = [jnp.exp2(v - top) for v in levels]
            whole = functools.reduce(jnp.add, shares)
            total = jnp.zeros((n, head_dim), F32)
            for p in range(parts):
                flat = jnp.broadcast_to(shares[p] / whole, (n, 128))
                share = jnp.sum(jnp.where(eye[:n], flat, 0.0), axis=1, keepdims=True)
                total = total + share * part_ref[p, t * 128 : t * 128 + n, cols].astype(F32)
            outs.append(total.astype(BF16))
        pieces.append(jnp.concatenate(outs, axis=0))
    attn = jnp.concatenate(pieces, axis=1)
    for c in range(w_ref.shape[1] // 512):
        at = pl.ds(c * 512, 512)
        o_ref[:, at] = jnp.dot(attn, w_ref[:, at], preferred_element_type=F32).astype(BF16)


def project(parts, weight):
    rows = parts.shape[1] - STAT_ROWS
    return pl.pallas_call(
        project_kernel,
        out_shape=jax.ShapeDtypeStruct((rows, weight.shape[1]), BF16),
        cost_estimate=pl.CostEstimate(
            flops=2 * rows * weight.size, bytes_accessed=3 * 2**20, transcendentals=0
        ),
        name="project",
    )(parts, weight)


def feed(x, weights, units):
    gate = jnp.dot(x, weights[:, 0:units], preferred_element_type=F32)
    up = jnp.dot(x, weights[:, units : 2 * units], preferred_element_type=F32)
    hidden = (jax.nn.silu(gate) * up).astype(BF16)
    return lax.dot_general(
        hidden,
        weights[:, 2 * units : 3 * units],
        (((1,), (1,)), ((), ())),
        preferred_element_type=F32,
    ).astype(BF16)


def normalize(stream, gain):
    values = stream.astype(F32)
    return (
        values * lax.rsqrt(jnp.mean(values * values, axis=-1, keepdims=True) + EPSILON) * gain
    ).astype(BF16)


def summed_over_tp(x):
    share = x.shape[0] // lax.axis_size("tp")
    blocks = lax.all_to_all(x.reshape(-1, share, x.shape[1]), "tp", 0, 0, tiled=True)
    return jnp.sum(blocks.astype(F32), axis=0)


def body(
    resid,
    query,
    key,
    value,
    q_gain,
    k_gain,
    out_weight,
    norm_gain,
    gate_weight,
    up_weight,
    down_weight,
):
    rows = query.shape[0]
    units = gate_weight.shape[1]
    shard = [gate_weight, up_weight, down_weight.T]
    weights = lax.all_gather(jnp.concatenate(shard, axis=1), SP, axis=0, tiled=True)

    copies, keys_values = prep(query, key, value, q_gain, k_gain, lax.axis_size("sp_1"))
    queries = lax.all_to_all(copies, "sp_1", 0, 0, tiled=True)
    keys_values = lax.all_gather(keys_values, "sp_0", axis=0, tiled=True)
    partial = attend(queries, keys_values)
    partial = lax.all_to_all(partial, "sp_1", 0, 0, tiled=True)
    proj = summed_over_tp(project(partial, out_weight))
    share = rows // lax.axis_size("tp")
    my_resid = lax.dynamic_slice_in_dim(resid, lax.axis_index("tp") * share, share, 0)
    my_stream = (my_resid.astype(F32) + proj).astype(BF16)
    normed = lax.all_gather(normalize(my_stream, norm_gain), "tp", axis=0, tiled=True)
    down = summed_over_tp(feed(normed, weights, units))
    return (my_stream.astype(F32) + 0.5 * down).astype(BF16)


def solution(mesh):
    torus = Mesh(mesh.devices.reshape(8, 8, mesh.shape["tp"]), ("sp_0", "sp_1", "tp"))
    return jax.shard_map(
        body,
        mesh=torus,
        in_specs=(
            P(SP, None),
            P(SP, "tp"),
            P(SP, "tp"),
            P(SP, "tp"),
            P(),
            P(),
            P("tp", None),
            P(),
            P(SP, "tp"),
            P(SP, "tp"),
            P("tp", SP),
        ),
        out_specs=P(SP_TP, None),
        check_vma=False,
    )
```

```python
import functools

import jax
import jax.numpy as jnp
import numpy as np
from jax import lax
from jax.experimental import pallas as pl
from jax.experimental.pallas import tpu as pltpu
from jax.sharding import Mesh
from jax.sharding import PartitionSpec as P

GRID_W = 64
SP = ("sp_0", "sp_1")
SP_TP = ("sp_0", "sp_1", "tp")
EPSILON = 1e-06
BF16 = jnp.bfloat16
F32 = jnp.float32
ROPE_BASE = 10000.0
STAT_ROWS = 16
LOG2E = 1.4426950408889634


def rope_tables(head_dim):
    quarter = head_dim // 4
    lane = np.arange(head_dim)
    inverse = np.power(np.float32(ROPE_BASE), -(lane % quarter).astype(np.float32) / np.float32(quarter))
    inverse = inverse.astype(np.float32)
    angles = np.arange(GRID_W, dtype=np.float32)[:, None] * inverse[None, :]
    sign = np.where((lane // quarter) % 2 == 0, -1.0, 1.0).astype(np.float32)
    cosine = np.cos(angles.astype(np.float64)).astype(np.float32)
    sine = np.sin(angles.astype(np.float64)).astype(np.float32) * sign
    return inverse[None, :], sign[None, :], cosine, sine


def prep_kernel(q_ref, k_ref, v_ref, qg_ref, kg_ref, inv_ref, sign_ref, cos_ref, sin_ref, qo_ref, kvo_ref):
    rows, head_dim = k_ref.shape
    heads = q_ref.shape[1] // head_dim
    quarter = head_dim // 4
    spans = rows // GRID_W
    sp = lax.axis_index("sp_0") * lax.axis_size("sp_1") + lax.axis_index("sp_1")
    first_row = (sp * spans).astype(F32)
    line = first_row + lax.broadcasted_iota(jnp.int32, (8, head_dim), 0).astype(F32)
    angle = line * inv_ref[...]
    row_cos = jnp.cos(angle)
    row_sin = jnp.sin(angle) * sign_ref[...]
    lane = lax.broadcasted_iota(jnp.int32, (GRID_W, head_dim), 1)
    by_row = lane < 2 * quarter
    is_first = (lane // quarter) % 2 == 0

    def turned(x, gain, cosine, sine):
        x = x.astype(F32)
        x = x * lax.rsqrt(jnp.mean(x * x, axis=-1, keepdims=True) + EPSILON) * gain
        other = jnp.where(
            is_first,
            pltpu.roll(x, head_dim - quarter, 1),
            pltpu.roll(x, quarter, 1),
        )
        return (x * cosine + other * sine).astype(BF16)

    for j in range(spans):
        at = pl.ds(j * GRID_W, GRID_W)
        cosine = jnp.where(by_row, row_cos[j : j + 1, :], cos_ref[...])
        sine = jnp.where(by_row, row_sin[j : j + 1, :], sin_ref[...])
        for h in range(heads):
            cols = slice(h * head_dim, (h + 1) * head_dim)
            made = turned(q_ref[at, cols], qg_ref[...], cosine, sine)
            for n in range(qo_ref.shape[0]):
                qo_ref[n, at, cols] = made
        kvo_ref[at, 0:head_dim] = turned(k_ref[at, :], kg_ref[...], cosine, sine)
    kvo_ref[:, head_dim:] = v_ref[...]


def prep(query, key, value, q_gain, k_gain, copies):
    rows, head_dim = key.shape
    inverse, sign, cosine, sine = rope_tables(head_dim)
    return pl.pallas_call(
        prep_kernel,
        out_shape=(
            jax.ShapeDtypeStruct((copies, *query.shape), BF16),
            jax.ShapeDtypeStruct((rows, 2 * head_dim), BF16),
        ),
        name="prep",
    )(
        query,
        key,
        value,
        q_gain.reshape(1, -1),
        k_gain.reshape(1, -1),
        jnp.asarray(inverse),
        jnp.asarray(sign),
        jnp.asarray(cosine),
        jnp.asarray(sine),
    )


def split3(x):
    a = x.astype(BF16)
    rest = x - a.astype(F32)
    b = rest.astype(BF16)
    c = (rest - b.astype(F32)).astype(BF16)
    return a, b, c


def packed_stats(level):
    rows = level.shape[0]
    eye = (
        lax.broadcasted_iota(jnp.int32, (128, 128), 0)
        == lax.broadcasted_iota(jnp.int32, (128, 128), 1)
    )
    place = lax.broadcasted_iota(jnp.int32, (STAT_ROWS, 128), 0)
    out = jnp.zeros((STAT_ROWS, 128), F32)
    for t in range(-(-rows // 128)):
        n = min(128, rows - t * 128)
        spread = jnp.broadcast_to(level[t * 128 : t * 128 + n], (n, 128))
        flat = jnp.sum(jnp.where(eye[:n], spread, 0.0), axis=0, keepdims=True)
        for k, piece in enumerate(split3(flat)):
            out = jnp.where(place == 3 * t + k, piece.astype(F32), out)
    return out.astype(BF16)


def attend_kernel(q_ref, next_ref, kv_ref, o_ref, even_ref, odd_ref, top_ref, *, chunk):
    rows, head_dim = q_ref.shape[1:]
    count = kv_ref.shape[0] // chunk
    factor = head_dim ** (-0.5) * LOG2E

    def score(q, s_ref, c, peak):
        at = pl.ds(c * chunk, chunk)
        s = lax.dot_general(
            q, kv_ref[at, 0:head_dim], (((1,), (1,)), ((), ())), preferred_element_type=F32
        )
        s_ref[:, at] = s
        for u in range(chunk // 128):
            x = s[:, u * 128 : (u + 1) * 128]
            peak = x if peak is None else jnp.maximum(peak, x)
        return peak

    def weigh(s_ref, top, c, total, accum):
        at = pl.ds(c * chunk, chunk)
        w = jnp.exp2((s_ref[:, at] - top) * factor)
        for u in range(chunk // 128):
            x = w[:, u * 128 : (u + 1) * 128]
            total = x if total is None else total + x
        d = jnp.dot(w.astype(BF16), kv_ref[at, head_dim:], preferred_element_type=F32)
        return total, d if accum is None else accum + d

    def finish(b, top, total, accum):
        whole = jnp.sum(total, axis=-1, keepdims=True)
        o_ref[b, 0:rows, :] = (accum / whole).astype(BF16)
        o_ref[b, rows:, :] = packed_stats(top * factor + jnp.log2(whole))

    @pl.when(pl.program_id(0) == 0)
    def _():
        peak = None
        for c in range(count):
            peak = score(q_ref[0], even_ref, c, peak)
        top_ref[...] = jnp.broadcast_to(jnp.max(peak, axis=-1, keepdims=True), top_ref.shape)

    top = top_ref[:, 0:1]
    for b, (q, s_ref, done_ref) in enumerate(
        ((q_ref[1], odd_ref, even_ref), (next_ref[0], even_ref, odd_ref))
    ):
        peak = total = accum = None
        for c in range(count):
            peak = score(q, s_ref, c, peak)
            total, accum = weigh(done_ref, top, c, total, accum)
        finish(b, top, total, accum)
        top = jnp.max(peak, axis=-1, keepdims=True)
    top_ref[...] = jnp.broadcast_to(top, top_ref.shape)


def attend(queries, keys_values, head):
    parts, rows, _ = queries.shape
    keys = keys_values.shape[0]
    head_dim = keys_values.shape[1] // 2
    steps = parts // 2
    work = parts * rows * keys
    return pl.pallas_call(
        functools.partial(attend_kernel, chunk=next(n for n in (512, 384, 256, 128) if keys % n == 0)),
        grid=(steps,),
        in_specs=[
            pl.BlockSpec((2, rows, head_dim), lambda i: (i, 0, head)),
            pl.BlockSpec(
                (2, rows, head_dim), lambda i: (jnp.minimum(i + 1, steps - 1), 0, head)
            ),
            pl.BlockSpec((keys, 2 * head_dim), lambda i: (0, 0)),
        ],
        out_specs=pl.BlockSpec((2, rows + STAT_ROWS, head_dim), lambda i: (i, 0, 0)),
        out_shape=jax.ShapeDtypeStruct((parts, rows + STAT_ROWS, head_dim), BF16),
        scratch_shapes=[
            pltpu.VMEM((rows, keys), F32),
            pltpu.VMEM((rows, keys), F32),
            pltpu.VMEM((rows, 128), F32),
        ],
        compiler_params=pltpu.CompilerParams(
            dimension_semantics=("arbitrary",), vmem_limit_bytes=32 * 2**20
        ),
        cost_estimate=pl.CostEstimate(
            flops=4 * work * head_dim, bytes_accessed=2 * 2**20, transcendentals=work
        ),
        name=f"attend{head}",
    )(queries, queries, keys_values)


def project_kernel(*refs):
    *part_refs, w_ref, o_ref = refs
    parts, all_rows, head_dim = part_refs[0].shape
    rows = all_rows - STAT_ROWS
    eye = (
        lax.broadcasted_iota(jnp.int32, (128, 128), 0)
        == lax.broadcasted_iota(jnp.int32, (128, 128), 1)
    )
    pieces = []
    for part_ref in part_refs:
        outs = []
        stats = [part_ref[p, rows:, :].astype(F32) for p in range(parts)]
        for t in range(-(-rows // 128)):
            n = min(128, rows - t * 128)
            levels = [
                s[3 * t : 3 * t + 1] + s[3 * t + 1 : 3 * t + 2] + s[3 * t + 2 : 3 * t + 3]
                for s in stats
            ]
            top = functools.reduce(jnp.maximum, levels)
            shares = [jnp.exp2(v - top) for v in levels]
            whole = functools.reduce(jnp.add, shares)
            total = jnp.zeros((n, head_dim), F32)
            for p in range(parts):
                flat = jnp.broadcast_to(shares[p] / whole, (n, 128))
                share = jnp.sum(jnp.where(eye[:n], flat, 0.0), axis=1, keepdims=True)
                total = total + share * part_ref[p, t * 128 : t * 128 + n, :].astype(F32)
            outs.append(total.astype(BF16))
        pieces.append(jnp.concatenate(outs, axis=0))
    attn = jnp.concatenate(pieces, axis=1)
    for c in range(w_ref.shape[1] // 512):
        at = pl.ds(c * 512, 512)
        o_ref[:, at] = jnp.dot(attn, w_ref[:, at], preferred_element_type=F32).astype(BF16)


def project(parts, weight):
    rows = parts[0].shape[1] - STAT_ROWS
    return pl.pallas_call(
        project_kernel,
        out_shape=jax.ShapeDtypeStruct((rows, weight.shape[1]), BF16),
        cost_estimate=pl.CostEstimate(
            flops=2 * rows * weight.size, bytes_accessed=3 * 2**20, transcendentals=0
        ),
        name="project",
    )(*parts, weight)


def feed_kernel(x_ref, w_hbm, o_ref, w_ref, acc_ref, sems, *, units):
    depth, width = w_ref.shape
    pieces = sems.shape[0]
    block = depth // pieces
    both = 2 * units
    spare = width - 3 * units
    copies = []
    for i in range(pieces):
        at = pl.ds(i * block, block)
        copies.append(pltpu.make_async_copy(w_hbm.at[at], w_ref.at[at], sems.at[i]))
        copies[-1].start()
    for i in range(pieces):
        at = pl.ds(i * block, block)
        copies[i].wait()
        part = jnp.dot(x_ref[:, at], w_ref[at, 0:both], preferred_element_type=F32)
        acc_ref[...] = part if i == 0 else acc_ref[...] + part
    gate = acc_ref[:, 0:units]
    up = acc_ref[:, units:both]
    hidden = (gate / (1.0 + jnp.exp(-gate)) * up).astype(BF16)
    if spare:
        hidden = jnp.concatenate([hidden, jnp.zeros((hidden.shape[0], spare), BF16)], axis=1)
    nt = (((1,), (1,)), ((), ()))
    for i in range(depth // 256):
        at = pl.ds(i * 256, 256)
        o_ref[:, at] = lax.dot_general(
            hidden, w_ref[at, both:], nt, preferred_element_type=F32
        ).astype(BF16)


def feed(x, weights, units):
    rows, depth = x.shape
    width = weights.shape[1]
    pieces = 8
    vmem = pl.BlockSpec(memory_space=pltpu.VMEM)
    return pl.pallas_call(
        functools.partial(feed_kernel, units=units),
        in_specs=[vmem, pl.BlockSpec(memory_space=pl.ANY)],
        out_specs=vmem,
        out_shape=jax.ShapeDtypeStruct((rows, depth), BF16),
        scratch_shapes=[
            pltpu.VMEM((depth, width), BF16),
            pltpu.VMEM((rows, 2 * units), F32),
            pltpu.SemaphoreType.DMA((pieces,)),
        ],
        compiler_params=pltpu.CompilerParams(vmem_limit_bytes=60 * 2**20),
        cost_estimate=pl.CostEstimate(
            flops=6 * rows * depth * units, bytes_accessed=10 * 2**20, transcendentals=0
        ),
        name="feed",
    )(x, weights)


def normalize(stream, gain):
    values = stream.astype(F32)
    return (
        values * lax.rsqrt(jnp.mean(values * values, axis=-1, keepdims=True) + EPSILON) * gain
    ).astype(BF16)


def summed_over_tp(x):
    share = x.shape[0] // lax.axis_size("tp")
    blocks = lax.all_to_all(x.reshape(-1, share, x.shape[1]), "tp", 0, 0, tiled=True)
    return jnp.sum(blocks.astype(F32), axis=0)


def body(
    resid,
    query,
    key,
    value,
    q_gain,
    k_gain,
    out_weight,
    norm_gain,
    gate_weight,
    up_weight,
    down_weight,
):
    rows = query.shape[0]
    units = gate_weight.shape[1]
    shard = [gate_weight, up_weight, down_weight.T]
    spare = -(3 * units) % 128
    if spare:
        shard.append(jnp.zeros((gate_weight.shape[0], spare), BF16))
    weights = lax.all_gather(jnp.concatenate(shard, axis=1), SP, axis=0, tiled=True)

    copies, keys_values = prep(query, key, value, q_gain, k_gain, lax.axis_size("sp_1"))
    queries = lax.all_to_all(copies, "sp_1", 0, 0, tiled=True)
    keys_values = lax.all_gather(keys_values, "sp_0", axis=0, tiled=True)
    partials = [
        lax.all_to_all(attend(queries, keys_values, h), "sp_1", 0, 0, tiled=True)
        for h in range(query.shape[1] // key.shape[1])
    ]
    proj = summed_over_tp(project(partials, out_weight))
    share = rows // lax.axis_size("tp")
    my_resid = lax.dynamic_slice_in_dim(resid, lax.axis_index("tp") * share, share, 0)
    my_stream = (my_resid.astype(F32) + proj).astype(BF16)
    normed = lax.all_gather(normalize(my_stream, norm_gain), "tp", axis=0, tiled=True)
    down = summed_over_tp(feed(normed, weights, units))
    return (my_stream.astype(F32) + 0.5 * down).astype(BF16)


def solution(mesh):
    torus = Mesh(mesh.devices.reshape(8, 8, mesh.shape["tp"]), ("sp_0", "sp_1", "tp"))
    return jax.shard_map(
        body,
        mesh=torus,
        in_specs=(
            P(SP, None),
            P(SP, "tp"),
            P(SP, "tp"),
            P(SP, "tp"),
            P(),
            P(),
            P("tp", None),
            P(),
            P(SP, "tp"),
            P(SP, "tp"),
            P("tp", SP),
        ),
        out_specs=P(SP_TP, None),
        check_vma=False,
    )
```

```python
import functools

import jax
import jax.numpy as jnp
import numpy as np
from jax import lax
from jax.experimental import pallas as pl
from jax.experimental.pallas import tpu as pltpu
from jax.sharding import Mesh
from jax.sharding import PartitionSpec as P

GRID_W = 64
SP = ("sp_0", "sp_1")
TP = ("x", "c")
EPSILON = 1e-06
BF16 = jnp.bfloat16
F32 = jnp.float32
ROPE_BASE = 10000.0
STAT_ROWS = 16
LOG2E = 1.4426950408889634


def rope_tables(head_dim):
    quarter = head_dim // 4
    lane = np.arange(head_dim)
    inverse = np.power(np.float32(ROPE_BASE), -(lane % quarter).astype(np.float32) / np.float32(quarter))
    inverse = inverse.astype(np.float32)
    angles = np.arange(GRID_W, dtype=np.float32)[:, None] * inverse[None, :]
    sign = np.where((lane // quarter) % 2 == 0, -1.0, 1.0).astype(np.float32)
    cosine = np.cos(angles.astype(np.float64)).astype(np.float32)
    sine = np.sin(angles.astype(np.float64)).astype(np.float32) * sign
    return inverse[None, :], sign[None, :], cosine, sine


def prep_kernel(q_ref, k_ref, v_ref, qg_ref, kg_ref, inv_ref, sign_ref, cos_ref, sin_ref, qo_ref, kvo_ref):
    rows, head_dim = k_ref.shape
    heads = q_ref.shape[1] // head_dim
    quarter = head_dim // 4
    spans = rows // GRID_W
    sp = lax.axis_index("sp_0") * lax.axis_size("sp_1") + lax.axis_index("sp_1")
    first_row = (sp * spans).astype(F32)
    line = first_row + lax.broadcasted_iota(jnp.int32, (8, head_dim), 0).astype(F32)
    angle = line * inv_ref[...]
    row_cos = jnp.cos(angle)
    row_sin = jnp.sin(angle) * sign_ref[...]
    lane = lax.broadcasted_iota(jnp.int32, (GRID_W, head_dim), 1)
    by_row = lane < 2 * quarter
    is_first = (lane // quarter) % 2 == 0

    def turned(x, gain, cosine, sine):
        x = x.astype(F32)
        x = x * lax.rsqrt(jnp.mean(x * x, axis=-1, keepdims=True) + EPSILON) * gain
        other = jnp.where(
            is_first,
            pltpu.roll(x, head_dim - quarter, 1),
            pltpu.roll(x, quarter, 1),
        )
        return (x * cosine + other * sine).astype(BF16)

    for j in range(spans):
        at = pl.ds(j * GRID_W, GRID_W)
        cosine = jnp.where(by_row, row_cos[j : j + 1, :], cos_ref[...])
        sine = jnp.where(by_row, row_sin[j : j + 1, :], sin_ref[...])
        for h in range(heads):
            cols = slice(h * head_dim, (h + 1) * head_dim)
            made = turned(q_ref[at, cols], qg_ref[...], cosine, sine)
            for n in range(qo_ref.shape[0]):
                qo_ref[n, at, cols] = made
        kvo_ref[at, 0:head_dim] = turned(k_ref[at, :], kg_ref[...], cosine, sine)
    kvo_ref[:, head_dim:] = v_ref[...]


def prep(query, key, value, q_gain, k_gain, copies):
    rows, head_dim = key.shape
    inverse, sign, cosine, sine = rope_tables(head_dim)
    return pl.pallas_call(
        prep_kernel,
        out_shape=(
            jax.ShapeDtypeStruct((copies, *query.shape), BF16),
            jax.ShapeDtypeStruct((rows, 2 * head_dim), BF16),
        ),
        name="prep",
    )(
        query,
        key,
        value,
        q_gain.reshape(1, -1),
        k_gain.reshape(1, -1),
        jnp.asarray(inverse),
        jnp.asarray(sign),
        jnp.asarray(cosine),
        jnp.asarray(sine),
    )


def split3(x):
    a = x.astype(BF16)
    rest = x - a.astype(F32)
    b = rest.astype(BF16)
    c = (rest - b.astype(F32)).astype(BF16)
    return a, b, c


def packed_stats(level):
    rows = level.shape[0]
    eye = (
        lax.broadcasted_iota(jnp.int32, (128, 128), 0)
        == lax.broadcasted_iota(jnp.int32, (128, 128), 1)
    )
    place = lax.broadcasted_iota(jnp.int32, (STAT_ROWS, 128), 0)
    out = jnp.zeros((STAT_ROWS, 128), F32)
    for t in range(-(-rows // 128)):
        n = min(128, rows - t * 128)
        spread = jnp.broadcast_to(level[t * 128 : t * 128 + n], (n, 128))
        flat = jnp.sum(jnp.where(eye[:n], spread, 0.0), axis=0, keepdims=True)
        for k, piece in enumerate(split3(flat)):
            out = jnp.where(place == 3 * t + k, piece.astype(F32), out)
    return out.astype(BF16)


def attend_kernel(q_ref, next_ref, kv_ref, o_ref, even_ref, odd_ref, top_ref, *, chunk):
    rows = q_ref.shape[1]
    head_dim = q_ref.shape[2] // 2
    count = kv_ref.shape[0] // chunk
    factor = head_dim ** (-0.5) * LOG2E

    def score(q, s_ref, c, peak):
        at = pl.ds(c * chunk, chunk)
        s = lax.dot_general(
            q, kv_ref[at, 0:head_dim], (((1,), (1,)), ((), ())), preferred_element_type=F32
        )
        s_ref[:, at] = s
        for u in range(chunk // 128):
            x = s[:, u * 128 : (u + 1) * 128]
            peak = x if peak is None else jnp.maximum(peak, x)
        return peak

    def weigh(s_ref, top, c, total, accum):
        at = pl.ds(c * chunk, chunk)
        w = jnp.exp2((s_ref[:, at] - top) * factor)
        for u in range(chunk // 128):
            x = w[:, u * 128 : (u + 1) * 128]
            total = x if total is None else total + x
        d = jnp.dot(w.astype(BF16), kv_ref[at, head_dim:], preferred_element_type=F32)
        return total, d if accum is None else accum + d

    def finish(b, top, total, accum):
        whole = jnp.sum(total, axis=-1, keepdims=True)
        cols = slice(b * head_dim, (b + 1) * head_dim)
        o_ref[0, 0:rows, cols] = (accum / whole).astype(BF16)
        o_ref[0, rows:, cols] = packed_stats(top * factor + jnp.log2(whole))

    @pl.when(pl.program_id(0) == 0)
    def _():
        peak = None
        for c in range(count):
            peak = score(q_ref[0, :, 0:head_dim], even_ref, c, peak)
        top_ref[...] = jnp.broadcast_to(jnp.max(peak, axis=-1, keepdims=True), top_ref.shape)

    top = top_ref[:, 0:1]
    for b, (q, s_ref, done_ref) in enumerate(
        ((q_ref[0, :, head_dim:], odd_ref, even_ref), (next_ref[0, :, 0:head_dim], even_ref, odd_ref))
    ):
        peak = total = accum = None
        for c in range(count):
            peak = score(q, s_ref, c, peak)
            total, accum = weigh(done_ref, top, c, total, accum)
        finish(b, top, total, accum)
        top = jnp.max(peak, axis=-1, keepdims=True)
    top_ref[...] = jnp.broadcast_to(top, top_ref.shape)


def attend(queries, keys_values):
    parts, rows, width = queries.shape
    keys = keys_values.shape[0]
    head_dim = width // 2
    work = parts * 2 * rows * keys
    return pl.pallas_call(
        functools.partial(
            attend_kernel, chunk=next(n for n in (512, 384, 256, 128) if keys % n == 0)
        ),
        grid=(parts,),
        in_specs=[
            pl.BlockSpec((1, rows, width), lambda i: (i, 0, 0)),
            pl.BlockSpec((1, rows, width), lambda i: (jnp.minimum(i + 1, parts - 1), 0, 0)),
            pl.BlockSpec((keys, 2 * head_dim), lambda i: (0, 0)),
        ],
        out_specs=pl.BlockSpec((1, rows + STAT_ROWS, width), lambda i: (i, 0, 0)),
        out_shape=jax.ShapeDtypeStruct((parts, rows + STAT_ROWS, width), BF16),
        scratch_shapes=[
            pltpu.VMEM((rows, keys), F32),
            pltpu.VMEM((rows, keys), F32),
            pltpu.VMEM((rows, 128), F32),
        ],
        compiler_params=pltpu.CompilerParams(
            dimension_semantics=("arbitrary",), vmem_limit_bytes=32 * 2**20
        ),
        cost_estimate=pl.CostEstimate(
            flops=4 * work * head_dim, bytes_accessed=4 * 2**20, transcendentals=work
        ),
        name="attend",
    )(queries, queries, keys_values)


def combine_kernel(part_ref, o_ref):
    parts, all_rows, width = part_ref.shape
    rows = all_rows - STAT_ROWS
    cores, held = o_ref.shape[:2]
    share = rows // lax.axis_size(TP)
    eye = (
        lax.broadcasted_iota(jnp.int32, (128, 128), 0)
        == lax.broadcasted_iota(jnp.int32, (128, 128), 1)
    )
    for h in range(width // 128):
        cols = slice(h * 128, (h + 1) * 128)
        stats = [part_ref[p, rows:, cols].astype(F32) for p in range(parts)]
        outs = []
        for t in range(-(-rows // 128)):
            n = min(128, rows - t * 128)
            levels = [
                s[3 * t : 3 * t + 1] + s[3 * t + 1 : 3 * t + 2] + s[3 * t + 2 : 3 * t + 3]
                for s in stats
            ]
            top = functools.reduce(jnp.maximum, levels)
            shares = [jnp.exp2(v - top) for v in levels]
            whole = functools.reduce(jnp.add, shares)
            total = jnp.zeros((n, 128), F32)
            for p in range(parts):
                flat = jnp.broadcast_to(shares[p] / whole, (n, 128))
                portion = jnp.sum(jnp.where(eye[:n], flat, 0.0), axis=1, keepdims=True)
                total = total + portion * part_ref[p, t * 128 : t * 128 + n, cols].astype(F32)
            outs.append(total)
        attn = jnp.concatenate(outs, axis=0)
        for k in range(rows // share):
            at = pl.ds(k // cores * share, share)
            o_ref[k % cores, at, cols] = attn[k * share : (k + 1) * share].astype(BF16)


def combine(parts):
    rows = parts.shape[1] - STAT_ROWS
    cores = lax.axis_size("c")
    return pl.pallas_call(
        combine_kernel,
        out_shape=jax.ShapeDtypeStruct((cores, rows // cores, parts.shape[2]), BF16),
        compiler_params=pltpu.CompilerParams(vmem_limit_bytes=16 * 2**20),
        cost_estimate=pl.CostEstimate(
            flops=2 * parts.size, bytes_accessed=2**20, transcendentals=0
        ),
        name="combine",
    )(parts)


def project_kernel(x_ref, own_ref, other_ref, o_ref):
    me = lax.axis_index("c")
    mine = x_ref[me, me]
    others = x_ref[1 - me, me]
    for c in range(own_ref.shape[1] // 512):
        at = pl.ds(c * 512, 512)
        o_ref[:, at] = (
            jnp.dot(mine, own_ref[:, at], preferred_element_type=F32)
            + jnp.dot(others, other_ref[:, at], preferred_element_type=F32)
        ).astype(BF16)


def project(attn, own, other):
    rows = attn.shape[2]
    return pl.pallas_call(
        project_kernel,
        out_shape=jax.ShapeDtypeStruct((rows, own.shape[1]), BF16),
        compiler_params=pltpu.CompilerParams(vmem_limit_bytes=16 * 2**20),
        cost_estimate=pl.CostEstimate(
            flops=4 * rows * own.size, bytes_accessed=3 * 2**20, transcendentals=0
        ),
        name="project",
    )(attn, own, other)


def feed_kernel(x_ref, w_hbm, o_ref, w_ref, acc_ref, sems, *, units):
    depth, width = w_ref.shape
    pieces = sems.shape[0]
    block = depth // pieces
    both = 2 * units
    spare = width - 3 * units
    copies = []
    for i in range(pieces):
        at = pl.ds(i * block, block)
        copies.append(pltpu.make_async_copy(w_hbm.at[at], w_ref.at[at], sems.at[i]))
        copies[-1].start()
    for i in range(pieces):
        at = pl.ds(i * block, block)
        copies[i].wait()
        part = jnp.dot(x_ref[:, at], w_ref[at, 0:both], preferred_element_type=F32)
        acc_ref[...] = part if i == 0 else acc_ref[...] + part
    gate = acc_ref[:, 0:units]
    up = acc_ref[:, units:both]
    hidden = (gate / (1.0 + jnp.exp(-gate)) * up).astype(BF16)
    if spare:
        hidden = jnp.concatenate([hidden, jnp.zeros((hidden.shape[0], spare), BF16)], axis=1)
    nt = (((1,), (1,)), ((), ()))
    for i in range(depth // 256):
        at = pl.ds(i * 256, 256)
        o_ref[:, at] = lax.dot_general(
            hidden, w_ref[at, both:], nt, preferred_element_type=F32
        ).astype(BF16)


def feed(x, weights, units):
    rows, depth = x.shape
    width = weights.shape[1]
    pieces = 8
    vmem = pl.BlockSpec(memory_space=pltpu.VMEM)
    return pl.pallas_call(
        functools.partial(feed_kernel, units=units),
        in_specs=[vmem, pl.BlockSpec(memory_space=pl.ANY)],
        out_specs=vmem,
        out_shape=jax.ShapeDtypeStruct((rows, depth), BF16),
        scratch_shapes=[
            pltpu.VMEM((depth, width), BF16),
            pltpu.VMEM((rows, 2 * units), F32),
            pltpu.SemaphoreType.DMA((pieces,)),
        ],
        compiler_params=pltpu.CompilerParams(vmem_limit_bytes=60 * 2**20),
        cost_estimate=pl.CostEstimate(
            flops=6 * rows * depth * units, bytes_accessed=10 * 2**20, transcendentals=0
        ),
        name="feed",
    )(x, weights)


def normalize(stream, gain):
    values = stream.astype(F32)
    return (
        values * lax.rsqrt(jnp.mean(values * values, axis=-1, keepdims=True) + EPSILON) * gain
    ).astype(BF16)


def summed_over(x, axis):
    count = lax.axis_size(axis)
    blocks = lax.all_to_all(x.reshape(count, -1, x.shape[1]), axis, 0, 0, tiled=True)
    return jnp.sum(blocks.astype(F32), axis=0)


def body(
    resid,
    query,
    key,
    value,
    q_gain,
    k_gain,
    out_weight,
    norm_gain,
    gate_weight,
    up_weight,
    down_weight,
):
    rows = query.shape[0]
    units = gate_weight.shape[1]
    shard = [gate_weight, up_weight, down_weight.T]
    spare = -(3 * units) % 128
    if spare:
        shard.append(jnp.zeros((gate_weight.shape[0], spare), BF16))
    weights = lax.all_gather(jnp.concatenate(shard, axis=1), SP, axis=0, tiled=True)

    copies, keys_values = prep(query, key, value, q_gain, k_gain, lax.axis_size("sp_1"))
    queries = lax.all_to_all(copies, "sp_1", 0, 0, tiled=True)
    keys_values = lax.all_gather(keys_values, "sp_0", axis=0, tiled=True)
    other_weight = lax.ppermute(out_weight, "c", [(0, 1), (1, 0)])
    partial = lax.all_to_all(attend(queries, keys_values), "sp_1", 0, 0, tiled=True)
    attn = lax.all_gather(combine(partial), "c", axis=0)
    proj = summed_over(project(attn, out_weight, other_weight), "x")
    share = rows // lax.axis_size(TP)
    my_resid = lax.dynamic_slice_in_dim(resid, lax.axis_index(TP) * share, share, 0)
    my_stream = (my_resid.astype(F32) + proj).astype(BF16)
    normed = lax.all_gather(normalize(my_stream, norm_gain), TP, axis=0, tiled=True)
    down = summed_over(feed(normed, weights, units), TP)
    return (my_stream.astype(F32) + 0.5 * down).astype(BF16)


def solution(mesh):
    torus = Mesh(
        mesh.devices.reshape(8, 8, mesh.shape["tp"] // 2, 2), ("sp_0", "sp_1", "x", "c")
    )
    return jax.shard_map(
        body,
        mesh=torus,
        in_specs=(
            P(SP, None),
            P(SP, TP),
            P(SP, TP),
            P(SP, TP),
            P(),
            P(),
            P(TP, None),
            P(),
            P(SP, TP),
            P(SP, TP),
            P(TP, SP),
        ),
        out_specs=P(SP + TP, None),
        check_vma=False,
    )
```

```python
import functools

import jax
import jax.numpy as jnp
import numpy as np
from jax import lax
from jax.experimental import pallas as pl
from jax.experimental.pallas import tpu as pltpu
from jax.sharding import Mesh
from jax.sharding import PartitionSpec as P


GRID_W = 64
SP = ("sp_0", "ya", "yb")
ROW = ("ya", "yb")
FEED = ("x", "yb")
WEIGHTS = ("sp_0", "ya", "c")
TP = ("x", "c")
EPSILON = 1e-06
BF16 = jnp.bfloat16
F32 = jnp.float32
ROPE_BASE = 10000.0
STAT_ROWS = 16
LOG2E = 1.4426950408889634


def rope_tables(head_dim):
    quarter = head_dim // 4
    lane = np.arange(head_dim)
    inverse = np.power(np.float32(ROPE_BASE), -(lane % quarter).astype(np.float32) / np.float32(quarter))
    inverse = inverse.astype(np.float32)
    angles = np.arange(GRID_W, dtype=np.float32)[:, None] * inverse[None, :]
    sign = np.where((lane // quarter) % 2 == 0, -1.0, 1.0).astype(np.float32)
    cosine = np.cos(angles.astype(np.float64)).astype(np.float32)
    sine = np.sin(angles.astype(np.float64)).astype(np.float32) * sign
    return inverse[None, :], sign[None, :], cosine, sine


def prep_kernel(q_ref, k_ref, v_ref, qg_ref, kg_ref, inv_ref, sign_ref, cos_ref, sin_ref, qo_ref, kvo_ref):
    rows, head_dim = k_ref.shape
    heads = q_ref.shape[1] // head_dim
    quarter = head_dim // 4
    spans = rows // GRID_W
    sp = lax.axis_index("sp_0")
    for axis in ROW:
        sp = sp * lax.axis_size(axis) + lax.axis_index(axis)
    first_row = (sp * spans).astype(F32)
    line = first_row + lax.broadcasted_iota(jnp.int32, (8, head_dim), 0).astype(F32)
    angle = line * inv_ref[...]
    row_cos = jnp.cos(angle)
    row_sin = jnp.sin(angle) * sign_ref[...]
    lane = lax.broadcasted_iota(jnp.int32, (GRID_W, head_dim), 1)
    by_row = lane < 2 * quarter
    is_first = (lane // quarter) % 2 == 0

    def turned(x, gain, cosine, sine):
        x = x.astype(F32)
        x = x * lax.rsqrt(jnp.mean(x * x, axis=-1, keepdims=True) + EPSILON) * gain
        other = jnp.where(
            is_first,
            pltpu.roll(x, head_dim - quarter, 1),
            pltpu.roll(x, quarter, 1),
        )
        return (x * cosine + other * sine).astype(BF16)

    for j in range(spans):
        at = pl.ds(j * GRID_W, GRID_W)
        cosine = jnp.where(by_row, row_cos[j : j + 1, :], cos_ref[...])
        sine = jnp.where(by_row, row_sin[j : j + 1, :], sin_ref[...])
        for h in range(heads):
            cols = slice(h * head_dim, (h + 1) * head_dim)
            made = turned(q_ref[at, cols], qg_ref[...], cosine, sine)
            for n in range(qo_ref.shape[0]):
                qo_ref[n, at, cols] = made
        kvo_ref[at, 0:head_dim] = turned(k_ref[at, :], kg_ref[...], cosine, sine)
    kvo_ref[:, head_dim:] = v_ref[...]


def prep(query, key, value, q_gain, k_gain, copies):
    rows, head_dim = key.shape
    inverse, sign, cosine, sine = rope_tables(head_dim)
    return pl.pallas_call(
        prep_kernel,
        out_shape=(
            jax.ShapeDtypeStruct((copies, *query.shape), BF16),
            jax.ShapeDtypeStruct((rows, 2 * head_dim), BF16),
        ),
        cost_estimate=pl.CostEstimate(
            flops=4 * 10**9, bytes_accessed=2 * 2**20, transcendentals=0
        ),
        name="prep",
    )(
        query,
        key,
        value,
        q_gain.reshape(1, -1),
        k_gain.reshape(1, -1),
        jnp.asarray(inverse),
        jnp.asarray(sign),
        jnp.asarray(cosine),
        jnp.asarray(sine),
    )


def split3(x):
    a = x.astype(BF16)
    rest = x - a.astype(F32)
    b = rest.astype(BF16)
    c = (rest - b.astype(F32)).astype(BF16)
    return a, b, c


def packed_stats(level):
    rows = level.shape[0]
    eye = (
        lax.broadcasted_iota(jnp.int32, (128, 128), 0)
        == lax.broadcasted_iota(jnp.int32, (128, 128), 1)
    )
    place = lax.broadcasted_iota(jnp.int32, (STAT_ROWS, 128), 0)
    out = jnp.zeros((STAT_ROWS, 128), F32)
    for t in range(-(-rows // 128)):
        n = min(128, rows - t * 128)
        spread = jnp.broadcast_to(level[t * 128 : t * 128 + n], (n, 128))
        flat = jnp.sum(jnp.where(eye[:n], spread, 0.0), axis=0, keepdims=True)
        for k, piece in enumerate(split3(flat)):
            out = jnp.where(place == 3 * t + k, piece.astype(F32), out)
    return out.astype(BF16)


def attend_kernel(q_ref, next_ref, kv_ref, o_ref, even_ref, odd_ref, top_ref, *, chunk):
    rows = q_ref.shape[1]
    head_dim = q_ref.shape[2] // 2
    count = kv_ref.shape[0] // chunk
    factor = head_dim ** (-0.5) * LOG2E

    def score(q, s_ref, c, peak):
        at = pl.ds(c * chunk, chunk)
        s = lax.dot_general(
            q, kv_ref[at, 0:head_dim], (((1,), (1,)), ((), ())), preferred_element_type=F32
        )
        s_ref[:, at] = s
        for u in range(chunk // 128):
            x = s[:, u * 128 : (u + 1) * 128]
            peak = x if peak is None else jnp.maximum(peak, x)
        return peak

    def weigh(s_ref, top, c, total, accum):
        at = pl.ds(c * chunk, chunk)
        w = jnp.exp2((s_ref[:, at] - top) * factor)
        for u in range(chunk // 128):
            x = w[:, u * 128 : (u + 1) * 128]
            total = x if total is None else total + x
        d = jnp.dot(w.astype(BF16), kv_ref[at, head_dim:], preferred_element_type=F32)
        return total, d if accum is None else accum + d

    def finish(b, top, total, accum):
        whole = jnp.sum(total, axis=-1, keepdims=True)
        cols = slice(b * head_dim, (b + 1) * head_dim)
        o_ref[0, 0:rows, cols] = (accum / whole).astype(BF16)
        o_ref[0, rows:, cols] = packed_stats(top * factor + jnp.log2(whole))

    @pl.when(pl.program_id(0) == 0)
    def _():
        peak = None
        for c in range(count):
            peak = score(q_ref[0, :, 0:head_dim], even_ref, c, peak)
        top_ref[...] = jnp.broadcast_to(jnp.max(peak, axis=-1, keepdims=True), top_ref.shape)

    top = top_ref[:, 0:1]
    for b, (q, s_ref, done_ref) in enumerate(
        ((q_ref[0, :, head_dim:], odd_ref, even_ref), (next_ref[0, :, 0:head_dim], even_ref, odd_ref))
    ):
        peak = total = accum = None
        for c in range(count):
            peak = score(q, s_ref, c, peak)
            total, accum = weigh(done_ref, top, c, total, accum)
        finish(b, top, total, accum)
        top = jnp.max(peak, axis=-1, keepdims=True)
    top_ref[...] = jnp.broadcast_to(top, top_ref.shape)


def attend(queries, keys_values):
    parts, rows, width = queries.shape
    keys = keys_values.shape[0]
    head_dim = width // 2
    work = parts * 2 * rows * keys
    return pl.pallas_call(
        functools.partial(
            attend_kernel, chunk=next(n for n in (512, 384, 256, 128) if keys % n == 0)
        ),
        grid=(parts,),
        in_specs=[
            pl.BlockSpec((1, rows, width), lambda i: (i, 0, 0)),
            pl.BlockSpec((1, rows, width), lambda i: (jnp.minimum(i + 1, parts - 1), 0, 0)),
            pl.BlockSpec((keys, 2 * head_dim), lambda i: (0, 0)),
        ],
        out_specs=pl.BlockSpec((1, rows + STAT_ROWS, width), lambda i: (i, 0, 0)),
        out_shape=jax.ShapeDtypeStruct((parts, rows + STAT_ROWS, width), BF16),
        scratch_shapes=[
            pltpu.VMEM((rows, keys), F32),
            pltpu.VMEM((rows, keys), F32),
            pltpu.VMEM((rows, 128), F32),
        ],
        compiler_params=pltpu.CompilerParams(
            dimension_semantics=("arbitrary",), vmem_limit_bytes=32 * 2**20
        ),
        cost_estimate=pl.CostEstimate(
            flops=4 * work * head_dim, bytes_accessed=4 * 2**20, transcendentals=work
        ),
        name="attend",
    )(queries, queries, keys_values)


def combine_kernel(part_ref, o_ref):
    parts, all_rows, width = part_ref.shape
    rows = all_rows - STAT_ROWS
    cores, _ = o_ref.shape[:2]
    share = rows // lax.axis_size(TP)
    eye = (
        lax.broadcasted_iota(jnp.int32, (128, 128), 0)
        == lax.broadcasted_iota(jnp.int32, (128, 128), 1)
    )
    for h in range(width // 128):
        cols = slice(h * 128, (h + 1) * 128)
        stats = [part_ref[p, rows:, cols].astype(F32) for p in range(parts)]
        outs = []
        for t in range(-(-rows // 128)):
            n = min(128, rows - t * 128)
            levels = [
                s[3 * t : 3 * t + 1] + s[3 * t + 1 : 3 * t + 2] + s[3 * t + 2 : 3 * t + 3]
                for s in stats
            ]
            top = functools.reduce(jnp.maximum, levels)
            shares = [jnp.exp2(v - top) for v in levels]
            whole = functools.reduce(jnp.add, shares)
            total = jnp.zeros((n, 128), F32)
            for p in range(parts):
                flat = jnp.broadcast_to(shares[p] / whole, (n, 128))
                portion = jnp.sum(jnp.where(eye[:n], flat, 0.0), axis=1, keepdims=True)
                total = total + portion * part_ref[p, t * 128 : t * 128 + n, cols].astype(F32)
            outs.append(total)
        attn = jnp.concatenate(outs, axis=0)
        for k in range(rows // share):
            at = pl.ds(k // cores * share, share)
            o_ref[k % cores, at, cols] = attn[k * share : (k + 1) * share].astype(BF16)


def combine(parts):
    rows = parts.shape[1] - STAT_ROWS
    cores = lax.axis_size("c")
    return pl.pallas_call(
        combine_kernel,
        out_shape=jax.ShapeDtypeStruct((cores, rows // cores, parts.shape[2]), BF16),
        compiler_params=pltpu.CompilerParams(vmem_limit_bytes=16 * 2**20),
        cost_estimate=pl.CostEstimate(
            flops=2 * parts.size, bytes_accessed=2**20, transcendentals=0
        ),
        name="combine",
    )(parts)


def project_kernel(x_ref, own_ref, other_ref, o_ref):
    me = lax.axis_index("c")
    mine = x_ref[me, me]
    others = x_ref[1 - me, me]
    for c in range(own_ref.shape[1] // 512):
        at = pl.ds(c * 512, 512)
        o_ref[:, at] = (
            jnp.dot(mine, own_ref[:, at], preferred_element_type=F32)
            + jnp.dot(others, other_ref[:, at], preferred_element_type=F32)
        ).astype(BF16)


def project(attn, own, other):
    rows = attn.shape[2]
    return pl.pallas_call(
        project_kernel,
        out_shape=jax.ShapeDtypeStruct((rows, own.shape[1]), BF16),
        compiler_params=pltpu.CompilerParams(vmem_limit_bytes=16 * 2**20),
        cost_estimate=pl.CostEstimate(
            flops=4 * rows * own.size, bytes_accessed=3 * 2**20, transcendentals=0
        ),
        name="project",
    )(attn, own, other)


def feed_kernel(x_ref, w_ref, o_ref, acc_ref, *, units):
    depth, width = w_ref.shape
    both = 2 * units
    spare = width - 3 * units
    acc_ref[...] = jnp.dot(x_ref[...], w_ref[:, 0:both], preferred_element_type=F32)
    gate = acc_ref[:, 0:units]
    up = acc_ref[:, units:both]
    hidden = (gate / (1.0 + jnp.exp(-gate)) * up).astype(BF16)
    if spare:
        hidden = jnp.concatenate([hidden, jnp.zeros((hidden.shape[0], spare), BF16)], axis=1)
    nt = (((1,), (1,)), ((), ()))
    for i in range(depth // 256):
        at = pl.ds(i * 256, 256)
        o_ref[:, at] = lax.dot_general(
            hidden, w_ref[at, both:], nt, preferred_element_type=F32
        ).astype(BF16)


def feed(x, weights, units):
    rows, depth = x.shape
    vmem = pl.BlockSpec(memory_space=pltpu.VMEM)
    return pl.pallas_call(
        functools.partial(feed_kernel, units=units),
        in_specs=[vmem, vmem],
        out_specs=vmem,
        out_shape=jax.ShapeDtypeStruct((rows, depth), BF16),
        scratch_shapes=[pltpu.VMEM((rows, 2 * units), F32)],
        compiler_params=pltpu.CompilerParams(vmem_limit_bytes=32 * 2**20),
        cost_estimate=pl.CostEstimate(
            flops=6 * rows * depth * units, bytes_accessed=10 * 2**20, transcendentals=0
        ),
        name="feed",
    )(x, weights)


def stream_kernel(part_ref, resid_ref, gain_ref, _, stream_ref, copies_ref):
    proj = part_ref[0].astype(F32)
    for n in range(1, part_ref.shape[0]):
        proj = proj + part_ref[n].astype(F32)
    stream = (resid_ref[...].astype(F32) + proj).astype(BF16)
    stream_ref[...] = stream
    values = stream.astype(F32)
    normed = values * lax.rsqrt(jnp.mean(values * values, axis=-1, keepdims=True) + EPSILON)
    normed = (normed * gain_ref[...]).astype(BF16)
    for n in range(copies_ref.shape[0]):
        copies_ref[n] = normed


def stream_rows(parts, resid, gain, weights, copies):
    vmem = pl.BlockSpec(memory_space=pltpu.VMEM)
    return pl.pallas_call(
        stream_kernel,
        in_specs=[vmem, vmem, vmem, vmem],
        out_specs=(vmem, vmem),
        out_shape=(
            jax.ShapeDtypeStruct(resid.shape, BF16),
            jax.ShapeDtypeStruct((copies, *resid.shape), BF16),
        ),
        compiler_params=pltpu.CompilerParams(vmem_limit_bytes=8 * 2**20),
        cost_estimate=pl.CostEstimate(
            flops=2 * 10**10, bytes_accessed=2**20, transcendentals=0
        ),
        name="stream",
    )(parts, resid, gain.reshape(1, -1), weights[0:8, 0:128])


def scattered(x, axis):
    count = lax.axis_size(axis)
    return lax.all_to_all(x.reshape(count, -1, x.shape[1]), axis, 0, 0, tiled=True)


def body(
    resid,
    query,
    key,
    value,
    q_gain,
    k_gain,
    out_weight,
    norm_gain,
    gate_weight,
    up_weight,
    down_weight,
):
    rows = query.shape[0]
    units = gate_weight.shape[1]
    shard = [gate_weight, up_weight, down_weight.T]
    spare = -(3 * units) % 128
    if spare:
        shard.append(jnp.zeros((gate_weight.shape[0], spare), BF16))
    shard = jnp.concatenate(shard, axis=1)
    shard = lax.ppermute(shard, ("yb", "c"), [(0, 0), (1, 2), (2, 1), (3, 3)])
    weights = lax.all_gather(shard, WEIGHTS, axis=0, tiled=True)

    copies, keys_values = prep(query, key, value, q_gain, k_gain, lax.axis_size(ROW))
    queries = lax.all_to_all(copies, ROW, 0, 0, tiled=True)
    keys_values = lax.all_gather(keys_values, "sp_0", axis=0, tiled=True)
    other_weight = lax.ppermute(out_weight, "c", [(0, 1), (1, 0)])
    partial = lax.all_to_all(attend(queries, keys_values), ROW, 0, 0, tiled=True)
    attn = lax.all_gather(combine(partial), "c", axis=0)
    parts = scattered(project(attn, out_weight, other_weight), "x")
    share = rows // lax.axis_size(TP)
    my_resid = lax.dynamic_slice_in_dim(resid, lax.axis_index(TP) * share, share, 0)
    my_stream, copies = stream_rows(
        parts, my_resid, norm_gain, weights, lax.axis_size(FEED)
    )
    normed = lax.all_to_all(copies, FEED, 0, 0, tiled=True).reshape(-1, resid.shape[1])
    down = jnp.sum(scattered(feed(normed, weights, units), FEED).astype(F32), axis=0)
    return (my_stream.astype(F32) + 0.5 * down).astype(BF16)


def solution(mesh):
    torus = Mesh(
        mesh.devices.reshape(8, 4, 2, mesh.shape["tp"] // 2, 2),
        ("sp_0", "ya", "yb", "x", "c"),
    )
    return jax.shard_map(
        body,
        mesh=torus,
        in_specs=(
            P(SP, None),
            P(SP, TP),
            P(SP, TP),
            P(SP, TP),
            P(),
            P(),
            P(TP, None),
            P(),
            P(SP, TP),
            P(SP, TP),
            P(TP, SP),
        ),
        out_specs=P(SP + TP, None),
        check_vma=False,
    )
```

```python
import functools

import jax
import jax.numpy as jnp
import numpy as np
from jax import lax
from jax.experimental import pallas as pl
from jax.experimental.pallas import tpu as pltpu
from jax.sharding import Mesh
from jax.sharding import PartitionSpec as P

GRID_W = 64
SP = ("sp_0", "sp_1")
TP = ("x", "c")
EPSILON = 1e-06
BF16 = jnp.bfloat16
F32 = jnp.float32
ROPE_BASE = 10000.0
STAT_ROWS = 16
LOG2E = 1.4426950408889634


def rope_tables(head_dim):
    quarter = head_dim // 4
    lane = np.arange(head_dim)
    inverse = np.power(np.float32(ROPE_BASE), -(lane % quarter).astype(np.float32) / np.float32(quarter))
    inverse = inverse.astype(np.float32)
    angles = np.arange(GRID_W, dtype=np.float32)[:, None] * inverse[None, :]
    sign = np.where((lane // quarter) % 2 == 0, -1.0, 1.0).astype(np.float32)
    cosine = np.cos(angles.astype(np.float64)).astype(np.float32)
    sine = np.sin(angles.astype(np.float64)).astype(np.float32) * sign
    return inverse[None, :], sign[None, :], cosine, sine


def prep_kernel(
    q_ref,
    k_ref,
    v_ref,
    gate_ref,
    up_ref,
    down_ref,
    qg_ref,
    kg_ref,
    inv_ref,
    sign_ref,
    cos_ref,
    sin_ref,
    wo_ref,
    qo_ref,
    kvo_ref,
):
    units = gate_ref.shape[1]
    for n, ref in enumerate((gate_ref, up_ref, down_ref)):
        wo_ref[:, n * units : (n + 1) * units] = ref[...]
    rows, head_dim = k_ref.shape
    heads = q_ref.shape[1] // head_dim
    quarter = head_dim // 4
    spans = rows // GRID_W
    sp = lax.axis_index("sp_0") * lax.axis_size("sp_1") + lax.axis_index("sp_1")
    first_row = (sp * spans).astype(F32)
    line = first_row + lax.broadcasted_iota(jnp.int32, (8, head_dim), 0).astype(F32)
    angle = line * inv_ref[...]
    row_cos = jnp.cos(angle)
    row_sin = jnp.sin(angle) * sign_ref[...]
    lane = lax.broadcasted_iota(jnp.int32, (GRID_W, head_dim), 1)
    by_row = lane < 2 * quarter
    is_first = (lane // quarter) % 2 == 0

    def turned(x, gain, cosine, sine):
        x = x.astype(F32)
        x = x * lax.rsqrt(jnp.mean(x * x, axis=-1, keepdims=True) + EPSILON) * gain
        other = jnp.where(
            is_first,
            pltpu.roll(x, head_dim - quarter, 1),
            pltpu.roll(x, quarter, 1),
        )
        return (x * cosine + other * sine).astype(BF16)

    for j in range(spans):
        at = pl.ds(j * GRID_W, GRID_W)
        cosine = jnp.where(by_row, row_cos[j : j + 1, :], cos_ref[...])
        sine = jnp.where(by_row, row_sin[j : j + 1, :], sin_ref[...])
        for h in range(heads):
            cols = slice(h * head_dim, (h + 1) * head_dim)
            made = turned(q_ref[at, cols], qg_ref[...], cosine, sine)
            for n in range(qo_ref.shape[0]):
                qo_ref[n, at, cols] = made
        kvo_ref[at, 0:head_dim] = turned(k_ref[at, :], kg_ref[...], cosine, sine)
    kvo_ref[:, head_dim:] = v_ref[...]


def prep(query, key, value, gate, up, down, q_gain, k_gain, copies):
    rows, head_dim = key.shape
    inverse, sign, cosine, sine = rope_tables(head_dim)
    return pl.pallas_call(
        prep_kernel,
        out_shape=(
            jax.ShapeDtypeStruct((gate.shape[0], 3 * gate.shape[1]), BF16),
            jax.ShapeDtypeStruct((copies, *query.shape), BF16),
            jax.ShapeDtypeStruct((rows, 2 * head_dim), BF16),
        ),
        name="prep",
    )(
        query,
        key,
        value,
        gate,
        up,
        down,
        q_gain.reshape(1, -1),
        k_gain.reshape(1, -1),
        jnp.asarray(inverse),
        jnp.asarray(sign),
        jnp.asarray(cosine),
        jnp.asarray(sine),
    )


def split3(x):
    a = x.astype(BF16)
    rest = x - a.astype(F32)
    b = rest.astype(BF16)
    c = (rest - b.astype(F32)).astype(BF16)
    return a, b, c


def packed_stats(level):
    rows = level.shape[0]
    eye = (
        lax.broadcasted_iota(jnp.int32, (128, 128), 0)
        == lax.broadcasted_iota(jnp.int32, (128, 128), 1)
    )
    place = lax.broadcasted_iota(jnp.int32, (STAT_ROWS, 128), 0)
    out = jnp.zeros((STAT_ROWS, 128), F32)
    for t in range(-(-rows // 128)):
        n = min(128, rows - t * 128)
        spread = jnp.broadcast_to(level[t * 128 : t * 128 + n], (n, 128))
        flat = jnp.sum(jnp.where(eye[:n], spread, 0.0), axis=0, keepdims=True)
        for k, piece in enumerate(split3(flat)):
            out = jnp.where(place == 3 * t + k, piece.astype(F32), out)
    return out.astype(BF16)


def attend_kernel(q_ref, next_ref, kv_ref, o_ref, even_ref, odd_ref, top_ref, *, chunk):
    rows = q_ref.shape[1]
    head_dim = q_ref.shape[2] // 2
    count = kv_ref.shape[0] // chunk
    factor = head_dim ** (-0.5) * LOG2E

    def score(q, s_ref, c, peak):
        at = pl.ds(c * chunk, chunk)
        s = lax.dot_general(
            q, kv_ref[at, 0:head_dim], (((1,), (1,)), ((), ())), preferred_element_type=F32
        )
        s_ref[:, at] = s
        for u in range(chunk // 128):
            x = s[:, u * 128 : (u + 1) * 128]
            peak = x if peak is None else jnp.maximum(peak, x)
        return peak

    def weigh(s_ref, top, c, total, accum):
        at = pl.ds(c * chunk, chunk)
        w = jnp.exp2((s_ref[:, at] - top) * factor)
        for u in range(chunk // 128):
            x = w[:, u * 128 : (u + 1) * 128]
            total = x if total is None else total + x
        d = jnp.dot(w.astype(BF16), kv_ref[at, head_dim:], preferred_element_type=F32)
        return total, d if accum is None else accum + d

    def finish(b, top, total, accum):
        whole = jnp.sum(total, axis=-1, keepdims=True)
        cols = slice(b * head_dim, (b + 1) * head_dim)
        o_ref[0, 0:rows, cols] = (accum / whole).astype(BF16)
        o_ref[0, rows:, cols] = packed_stats(top * factor + jnp.log2(whole))

    @pl.when(pl.program_id(0) == 0)
    def _():
        peak = None
        for c in range(count):
            peak = score(q_ref[0, :, 0:head_dim], even_ref, c, peak)
        top_ref[...] = jnp.broadcast_to(jnp.max(peak, axis=-1, keepdims=True), top_ref.shape)

    top = top_ref[:, 0:1]
    for b, (q, s_ref, done_ref) in enumerate(
        ((q_ref[0, :, head_dim:], odd_ref, even_ref), (next_ref[0, :, 0:head_dim], even_ref, odd_ref))
    ):
        peak = total = accum = None
        for c in range(count):
            peak = score(q, s_ref, c, peak)
            total, accum = weigh(done_ref, top, c, total, accum)
        finish(b, top, total, accum)
        top = jnp.max(peak, axis=-1, keepdims=True)
    top_ref[...] = jnp.broadcast_to(top, top_ref.shape)


def attend(queries, keys_values):
    parts, rows, width = queries.shape
    keys = keys_values.shape[0]
    head_dim = width // 2
    work = parts * 2 * rows * keys
    return pl.pallas_call(
        functools.partial(
            attend_kernel, chunk=next(n for n in (512, 384, 256, 128) if keys % n == 0)
        ),
        grid=(parts,),
        in_specs=[
            pl.BlockSpec((1, rows, width), lambda i: (i, 0, 0)),
            pl.BlockSpec((1, rows, width), lambda i: (jnp.minimum(i + 1, parts - 1), 0, 0)),
            pl.BlockSpec((keys, 2 * head_dim), lambda i: (0, 0)),
        ],
        out_specs=pl.BlockSpec((1, rows + STAT_ROWS, width), lambda i: (i, 0, 0)),
        out_shape=jax.ShapeDtypeStruct((parts, rows + STAT_ROWS, width), BF16),
        scratch_shapes=[
            pltpu.VMEM((rows, keys), F32),
            pltpu.VMEM((rows, keys), F32),
            pltpu.VMEM((rows, 128), F32),
        ],
        compiler_params=pltpu.CompilerParams(
            dimension_semantics=("arbitrary",), vmem_limit_bytes=32 * 2**20
        ),
        cost_estimate=pl.CostEstimate(
            flops=4 * work * head_dim, bytes_accessed=4 * 2**20, transcendentals=work
        ),
        name="attend",
    )(queries, queries, keys_values)


def combine_kernel(part_ref, o_ref):
    parts, all_rows, width = part_ref.shape
    rows = all_rows - STAT_ROWS
    cores, held = o_ref.shape[:2]
    share = rows // lax.axis_size(TP)
    eye = (
        lax.broadcasted_iota(jnp.int32, (128, 128), 0)
        == lax.broadcasted_iota(jnp.int32, (128, 128), 1)
    )
    for h in range(width // 128):
        cols = slice(h * 128, (h + 1) * 128)
        stats = [part_ref[p, rows:, cols].astype(F32) for p in range(parts)]
        outs = []
        for t in range(-(-rows // 128)):
            n = min(128, rows - t * 128)
            levels = [
                s[3 * t : 3 * t + 1] + s[3 * t + 1 : 3 * t + 2] + s[3 * t + 2 : 3 * t + 3]
                for s in stats
            ]
            top = functools.reduce(jnp.maximum, levels)
            shares = [jnp.exp2(v - top) for v in levels]
            whole = functools.reduce(jnp.add, shares)
            total = jnp.zeros((n, 128), F32)
            for p in range(parts):
                flat = jnp.broadcast_to(shares[p] / whole, (n, 128))
                portion = jnp.sum(jnp.where(eye[:n], flat, 0.0), axis=1, keepdims=True)
                total = total + portion * part_ref[p, t * 128 : t * 128 + n, cols].astype(F32)
            outs.append(total)
        attn = jnp.concatenate(outs, axis=0)
        for k in range(rows // share):
            at = pl.ds(k // cores * share, share)
            o_ref[k % cores, at, cols] = attn[k * share : (k + 1) * share].astype(BF16)


def combine(parts):
    rows = parts.shape[1] - STAT_ROWS
    cores = lax.axis_size("c")
    return pl.pallas_call(
        combine_kernel,
        out_shape=jax.ShapeDtypeStruct((cores, rows // cores, parts.shape[2]), BF16),
        compiler_params=pltpu.CompilerParams(vmem_limit_bytes=16 * 2**20),
        cost_estimate=pl.CostEstimate(
            flops=2 * parts.size, bytes_accessed=2**20, transcendentals=0
        ),
        name="combine",
    )(parts)


def project_kernel(x_ref, own_ref, other_ref, o_ref):
    me = lax.axis_index("c")
    mine = x_ref[me, me]
    others = x_ref[1 - me, me]
    for c in range(own_ref.shape[1] // 512):
        at = pl.ds(c * 512, 512)
        o_ref[:, at] = (
            jnp.dot(mine, own_ref[:, at], preferred_element_type=F32)
            + jnp.dot(others, other_ref[:, at], preferred_element_type=F32)
        ).astype(BF16)


def project(attn, own, other):
    rows = attn.shape[2]
    return pl.pallas_call(
        project_kernel,
        out_shape=jax.ShapeDtypeStruct((rows, own.shape[1]), BF16),
        compiler_params=pltpu.CompilerParams(vmem_limit_bytes=16 * 2**20),
        cost_estimate=pl.CostEstimate(
            flops=4 * rows * own.size, bytes_accessed=3 * 2**20, transcendentals=0
        ),
        name="project",
    )(attn, own, other)


def feed_kernel(x_hbm, w_hbm, o_ref, x_ref, w_ref, acc_ref, sems, *, units):
    depth, width = w_ref.shape
    pieces = sems.shape[0] - 1
    block = depth // pieces
    both = 2 * units
    spare = width - 3 * units
    copies = []
    for i in range(pieces):
        at = pl.ds(i * block, block)
        copies.append(pltpu.make_async_copy(w_hbm.at[at], w_ref.at[at], sems.at[i]))
        copies[-1].start()
    rows_copy = pltpu.make_async_copy(x_hbm, x_ref, sems.at[pieces])
    rows_copy.start()
    rows_copy.wait()
    for i in range(pieces):
        at = pl.ds(i * block, block)
        copies[i].wait()
        part = jnp.dot(x_ref[:, at], w_ref[at, 0:both], preferred_element_type=F32)
        acc_ref[...] = part if i == 0 else acc_ref[...] + part
    gate = acc_ref[:, 0:units]
    up = acc_ref[:, units:both]
    hidden = (gate / (1.0 + jnp.exp(-gate)) * up).astype(BF16)
    if spare:
        hidden = jnp.concatenate([hidden, jnp.zeros((hidden.shape[0], spare), BF16)], axis=1)
    nt = (((1,), (1,)), ((), ()))
    for i in range(depth // 256):
        at = pl.ds(i * 256, 256)
        o_ref[:, at] = lax.dot_general(
            hidden, w_ref[at, both:], nt, preferred_element_type=F32
        ).astype(BF16)


def feed(x, weights, units):
    rows, depth = x.shape
    width = weights.shape[1]
    pieces = 8
    return pl.pallas_call(
        functools.partial(feed_kernel, units=units),
        in_specs=[pl.BlockSpec(memory_space=pl.ANY)] * 2,
        out_specs=pl.BlockSpec(memory_space=pltpu.VMEM),
        out_shape=jax.ShapeDtypeStruct((rows, depth), BF16),
        scratch_shapes=[
            pltpu.VMEM((rows, depth), BF16),
            pltpu.VMEM((depth, width), BF16),
            pltpu.VMEM((rows, 2 * units), F32),
            pltpu.SemaphoreType.DMA((pieces + 1,)),
        ],
        compiler_params=pltpu.CompilerParams(vmem_limit_bytes=60 * 2**20),
        cost_estimate=pl.CostEstimate(
            flops=6 * rows * depth * units, bytes_accessed=10 * 2**20, transcendentals=0
        ),
        name="feed",
    )(x, weights)


def stream_kernel(part_ref, resid_ref, gain_ref, stream_ref, normed_ref):
    proj = part_ref[0].astype(F32)
    for n in range(1, part_ref.shape[0]):
        proj = proj + part_ref[n].astype(F32)
    stream = (resid_ref[...].astype(F32) + proj).astype(BF16)
    stream_ref[...] = stream
    values = stream.astype(F32)
    normed = values * lax.rsqrt(jnp.mean(values * values, axis=-1, keepdims=True) + EPSILON)
    normed_ref[...] = (normed * gain_ref[...]).astype(BF16)


def stream_rows(parts, resid, gain):
    return pl.pallas_call(
        stream_kernel,
        out_shape=(
            jax.ShapeDtypeStruct(resid.shape, BF16),
            jax.ShapeDtypeStruct(resid.shape, BF16),
        ),
        compiler_params=pltpu.CompilerParams(vmem_limit_bytes=8 * 2**20),
        cost_estimate=pl.CostEstimate(
            flops=8 * resid.size, bytes_accessed=2**20, transcendentals=0
        ),
        name="stream",
    )(parts, resid, gain.reshape(1, -1))


def scattered(x, axis):
    count = lax.axis_size(axis)
    return lax.all_to_all(x.reshape(count, -1, x.shape[1]), axis, 0, 0, tiled=True)


def body(
    resid,
    query,
    key,
    value,
    q_gain,
    k_gain,
    out_weight,
    norm_gain,
    gate_weight,
    up_weight,
    down_weight,
):
    rows = query.shape[0]
    units = gate_weight.shape[1]
    shard, copies, keys_values = prep(
        query,
        key,
        value,
        gate_weight,
        up_weight,
        down_weight.T,
        q_gain,
        k_gain,
        lax.axis_size("sp_1"),
    )
    weights = lax.all_gather(shard, SP, axis=0, tiled=True)
    queries = lax.all_to_all(copies, "sp_1", 0, 0, tiled=True)
    keys_values = lax.all_gather(keys_values, "sp_0", axis=0, tiled=True)
    other_weight = lax.ppermute(out_weight, "c", [(0, 1), (1, 0)])
    partial = lax.all_to_all(attend(queries, keys_values), "sp_1", 0, 0, tiled=True)
    attn = lax.all_gather(combine(partial), "c", axis=0)
    parts = scattered(project(attn, out_weight, other_weight), "x")
    share = rows // lax.axis_size(TP)
    my_resid = lax.dynamic_slice_in_dim(resid, lax.axis_index(TP) * share, share, 0)
    my_stream, normed = stream_rows(parts, my_resid, norm_gain)
    normed = lax.all_gather(normed, TP, axis=0, tiled=True)
    down = jnp.sum(scattered(feed(normed, weights, units), TP).astype(F32), axis=0)
    return (my_stream.astype(F32) + 0.5 * down).astype(BF16)


def solution(mesh):
    torus = Mesh(
        mesh.devices.reshape(8, 8, mesh.shape["tp"] // 2, 2), ("sp_0", "sp_1", "x", "c")
    )
    return jax.shard_map(
        body,
        mesh=torus,
        in_specs=(
            P(SP, None),
            P(SP, TP),
            P(SP, TP),
            P(SP, TP),
            P(),
            P(),
            P(TP, None),
            P(),
            P(SP, TP),
            P(SP, TP),
            P(TP, SP),
        ),
        out_specs=P(SP + TP, None),
        check_vma=False,
    )
```

```python
import functools

import jax
import jax.numpy as jnp
import numpy as np
from jax import lax
from jax.experimental import pallas as pl
from jax.experimental.pallas import tpu as pltpu
from jax.sharding import Mesh
from jax.sharding import PartitionSpec as P

GRID_W = 64
SP = ("sp_0", "sp_1")
TP = ("x", "c")
EPSILON = 1e-06
BF16 = jnp.bfloat16
F32 = jnp.float32
ROPE_BASE = 10000.0
STAT_ROWS = 16
LOG2E = 1.4426950408889634


def rope_tables(head_dim):
    quarter = head_dim // 4
    lane = np.arange(head_dim)
    inverse = np.power(np.float32(ROPE_BASE), -(lane % quarter).astype(np.float32) / np.float32(quarter))
    inverse = inverse.astype(np.float32)
    angles = np.arange(GRID_W, dtype=np.float32)[:, None] * inverse[None, :]
    sign = np.where((lane // quarter) % 2 == 0, -1.0, 1.0).astype(np.float32)
    cosine = np.cos(angles.astype(np.float64)).astype(np.float32)
    sine = np.sin(angles.astype(np.float64)).astype(np.float32) * sign
    return inverse[None, :], sign[None, :], cosine, sine


def prep_kernel(
    q_ref,
    k_ref,
    v_ref,
    gate_ref,
    up_ref,
    down_ref,
    qg_ref,
    kg_ref,
    inv_ref,
    sign_ref,
    cos_ref,
    sin_ref,
    wo_ref,
    qo_ref,
    kvo_ref,
):
    units = gate_ref.shape[1]
    for n, ref in enumerate((gate_ref, up_ref, down_ref)):
        wo_ref[:, n * units : (n + 1) * units] = ref[...]
    spare = wo_ref.shape[1] - 3 * units
    if spare:
        wo_ref[:, 3 * units :] = jnp.zeros((wo_ref.shape[0], spare), BF16)
    rows, head_dim = k_ref.shape
    heads = q_ref.shape[1] // head_dim
    quarter = head_dim // 4
    spans = rows // GRID_W
    sp = lax.axis_index("sp_0") * lax.axis_size("sp_1") + lax.axis_index("sp_1")
    first_row = (sp * spans).astype(F32)
    line = first_row + lax.broadcasted_iota(jnp.int32, (8, head_dim), 0).astype(F32)
    angle = line * inv_ref[...]
    row_cos = jnp.cos(angle)
    row_sin = jnp.sin(angle) * sign_ref[...]
    lane = lax.broadcasted_iota(jnp.int32, (GRID_W, head_dim), 1)
    by_row = lane < 2 * quarter
    is_first = (lane // quarter) % 2 == 0

    def turned(x, gain, cosine, sine):
        x = x.astype(F32)
        x = x * lax.rsqrt(jnp.mean(x * x, axis=-1, keepdims=True) + EPSILON) * gain
        other = jnp.where(
            is_first,
            pltpu.roll(x, head_dim - quarter, 1),
            pltpu.roll(x, quarter, 1),
        )
        return (x * cosine + other * sine).astype(BF16)

    for j in range(spans):
        at = pl.ds(j * GRID_W, GRID_W)
        cosine = jnp.where(by_row, row_cos[j : j + 1, :], cos_ref[...])
        sine = jnp.where(by_row, row_sin[j : j + 1, :], sin_ref[...])
        for h in range(heads):
            cols = slice(h * head_dim, (h + 1) * head_dim)
            made = turned(q_ref[at, cols], qg_ref[...], cosine, sine)
            for n in range(qo_ref.shape[0]):
                qo_ref[n, at, cols] = made
        kvo_ref[at, 0:head_dim] = turned(k_ref[at, :], kg_ref[...], cosine, sine)
    kvo_ref[:, head_dim:] = v_ref[...]


def prep(query, key, value, gate, up, down, q_gain, k_gain, copies):
    rows, head_dim = key.shape
    inverse, sign, cosine, sine = rope_tables(head_dim)
    return pl.pallas_call(
        prep_kernel,
        out_shape=(
            jax.ShapeDtypeStruct((gate.shape[0], -(-3 * gate.shape[1] // 128) * 128), BF16),
            jax.ShapeDtypeStruct((copies, *query.shape), BF16),
            jax.ShapeDtypeStruct((rows, 2 * head_dim), BF16),
        ),
        name="prep",
    )(
        query,
        key,
        value,
        gate,
        up,
        down,
        q_gain.reshape(1, -1),
        k_gain.reshape(1, -1),
        jnp.asarray(inverse),
        jnp.asarray(sign),
        jnp.asarray(cosine),
        jnp.asarray(sine),
    )


def split3(x):
    a = x.astype(BF16)
    rest = x - a.astype(F32)
    b = rest.astype(BF16)
    c = (rest - b.astype(F32)).astype(BF16)
    return a, b, c


def packed_stats(level):
    rows = level.shape[0]
    eye = (
        lax.broadcasted_iota(jnp.int32, (128, 128), 0)
        == lax.broadcasted_iota(jnp.int32, (128, 128), 1)
    )
    place = lax.broadcasted_iota(jnp.int32, (STAT_ROWS, 128), 0)
    out = jnp.zeros((STAT_ROWS, 128), F32)
    for t in range(-(-rows // 128)):
        n = min(128, rows - t * 128)
        spread = jnp.broadcast_to(level[t * 128 : t * 128 + n], (n, 128))
        flat = jnp.sum(jnp.where(eye[:n], spread, 0.0), axis=0, keepdims=True)
        for k, piece in enumerate(split3(flat)):
            out = jnp.where(place == 3 * t + k, piece.astype(F32), out)
    return out.astype(BF16)


def attend_kernel(q_ref, next_ref, kv_ref, o_ref, even_ref, odd_ref, top_ref, *, chunk):
    rows = q_ref.shape[1]
    head_dim = q_ref.shape[2] // 2
    count = kv_ref.shape[0] // chunk
    factor = head_dim ** (-0.5) * LOG2E

    def score(q, s_ref, c, peak):
        at = pl.ds(c * chunk, chunk)
        s = lax.dot_general(
            q, kv_ref[at, 0:head_dim], (((1,), (1,)), ((), ())), preferred_element_type=F32
        )
        s_ref[:, at] = s
        for u in range(chunk // 128):
            x = s[:, u * 128 : (u + 1) * 128]
            peak = x if peak is None else jnp.maximum(peak, x)
        return peak

    def weigh(s_ref, top, c, total, accum):
        at = pl.ds(c * chunk, chunk)
        w = jnp.exp2((s_ref[:, at] - top) * factor)
        for u in range(chunk // 128):
            x = w[:, u * 128 : (u + 1) * 128]
            total = x if total is None else total + x
        d = jnp.dot(w.astype(BF16), kv_ref[at, head_dim:], preferred_element_type=F32)
        return total, d if accum is None else accum + d

    def finish(b, top, total, accum):
        whole = jnp.sum(total, axis=-1, keepdims=True)
        cols = slice(b * head_dim, (b + 1) * head_dim)
        o_ref[0, 0:rows, cols] = (accum / whole).astype(BF16)
        o_ref[0, rows:, cols] = packed_stats(top * factor + jnp.log2(whole))

    @pl.when(pl.program_id(0) == 0)
    def _():
        peak = None
        for c in range(count):
            peak = score(q_ref[0, :, 0:head_dim], even_ref, c, peak)
        top_ref[...] = jnp.broadcast_to(jnp.max(peak, axis=-1, keepdims=True), top_ref.shape)

    top = top_ref[:, 0:1]
    for b, (q, s_ref, done_ref) in enumerate(
        ((q_ref[0, :, head_dim:], odd_ref, even_ref), (next_ref[0, :, 0:head_dim], even_ref, odd_ref))
    ):
        peak = total = accum = None
        for c in range(count):
            peak = score(q, s_ref, c, peak)
            total, accum = weigh(done_ref, top, c, total, accum)
        finish(b, top, total, accum)
        top = jnp.max(peak, axis=-1, keepdims=True)
    top_ref[...] = jnp.broadcast_to(top, top_ref.shape)


def attend(queries, keys_values):
    parts, rows, width = queries.shape
    keys = keys_values.shape[0]
    head_dim = width // 2
    work = parts * 2 * rows * keys
    return pl.pallas_call(
        functools.partial(
            attend_kernel, chunk=next(n for n in (512, 384, 256, 128) if keys % n == 0)
        ),
        grid=(parts,),
        in_specs=[
            pl.BlockSpec((1, rows, width), lambda i: (i, 0, 0)),
            pl.BlockSpec((1, rows, width), lambda i: (jnp.minimum(i + 1, parts - 1), 0, 0)),
            pl.BlockSpec((keys, 2 * head_dim), lambda i: (0, 0)),
        ],
        out_specs=pl.BlockSpec((1, rows + STAT_ROWS, width), lambda i: (i, 0, 0)),
        out_shape=jax.ShapeDtypeStruct((parts, rows + STAT_ROWS, width), BF16),
        scratch_shapes=[
            pltpu.VMEM((rows, keys), F32),
            pltpu.VMEM((rows, keys), F32),
            pltpu.VMEM((rows, 128), F32),
        ],
        compiler_params=pltpu.CompilerParams(
            dimension_semantics=("arbitrary",), vmem_limit_bytes=32 * 2**20
        ),
        cost_estimate=pl.CostEstimate(
            flops=4 * work * head_dim, bytes_accessed=4 * 2**20, transcendentals=work
        ),
        name="attend",
    )(queries, queries, keys_values)


def combine_kernel(part_ref, o_ref):
    parts, all_rows, width = part_ref.shape
    rows = all_rows - STAT_ROWS
    cores, held = o_ref.shape[:2]
    share = rows // lax.axis_size(TP)
    eye = (
        lax.broadcasted_iota(jnp.int32, (128, 128), 0)
        == lax.broadcasted_iota(jnp.int32, (128, 128), 1)
    )
    for h in range(width // 128):
        cols = slice(h * 128, (h + 1) * 128)
        stats = [part_ref[p, rows:, cols].astype(F32) for p in range(parts)]
        outs = []
        for t in range(-(-rows // 128)):
            n = min(128, rows - t * 128)
            levels = [
                s[3 * t : 3 * t + 1] + s[3 * t + 1 : 3 * t + 2] + s[3 * t + 2 : 3 * t + 3]
                for s in stats
            ]
            top = functools.reduce(jnp.maximum, levels)
            shares = [jnp.exp2(v - top) for v in levels]
            whole = functools.reduce(jnp.add, shares)
            total = jnp.zeros((n, 128), F32)
            for p in range(parts):
                flat = jnp.broadcast_to(shares[p] / whole, (n, 128))
                portion = jnp.sum(jnp.where(eye[:n], flat, 0.0), axis=1, keepdims=True)
                total = total + portion * part_ref[p, t * 128 : t * 128 + n, cols].astype(F32)
            outs.append(total)
        attn = jnp.concatenate(outs, axis=0)
        for k in range(rows // share):
            at = pl.ds(k // cores * share, share)
            o_ref[k % cores, at, cols] = attn[k * share : (k + 1) * share].astype(BF16)


def combine(parts):
    rows = parts.shape[1] - STAT_ROWS
    cores = lax.axis_size("c")
    return pl.pallas_call(
        combine_kernel,
        out_shape=jax.ShapeDtypeStruct((cores, rows // cores, parts.shape[2]), BF16),
        compiler_params=pltpu.CompilerParams(vmem_limit_bytes=16 * 2**20),
        cost_estimate=pl.CostEstimate(
            flops=2 * parts.size, bytes_accessed=2**20, transcendentals=0
        ),
        name="combine",
    )(parts)


def project_kernel(x_ref, own_ref, other_ref, o_ref):
    me = lax.axis_index("c")
    mine = x_ref[me, me]
    others = x_ref[1 - me, me]
    for c in range(own_ref.shape[1] // 512):
        at = pl.ds(c * 512, 512)
        o_ref[:, at] = (
            jnp.dot(mine, own_ref[:, at], preferred_element_type=F32)
            + jnp.dot(others, other_ref[:, at], preferred_element_type=F32)
        ).astype(BF16)


def project(attn, own, other):
    rows = attn.shape[2]
    return pl.pallas_call(
        project_kernel,
        out_shape=jax.ShapeDtypeStruct((rows, own.shape[1]), BF16),
        compiler_params=pltpu.CompilerParams(vmem_limit_bytes=16 * 2**20),
        cost_estimate=pl.CostEstimate(
            flops=4 * rows * own.size, bytes_accessed=3 * 2**20, transcendentals=0
        ),
        name="project",
    )(attn, own, other)


def feed_kernel(x_hbm, w_hbm, o_ref, x_ref, w_ref, acc_ref, sems, *, units):
    depth, width = w_ref.shape
    pieces = sems.shape[0] - 1
    block = depth // pieces
    both = 2 * units
    spare = width - 3 * units
    rows_copy = pltpu.make_async_copy(x_hbm, x_ref, sems.at[pieces])
    rows_copy.start()
    copies = []
    for i in range(pieces):
        at = pl.ds(i * block, block)
        copies.append(pltpu.make_async_copy(w_hbm.at[at], w_ref.at[at], sems.at[i]))
        copies[-1].start()
    rows_copy.wait()
    for i in range(pieces):
        at = pl.ds(i * block, block)
        copies[i].wait()
        part = jnp.dot(x_ref[:, at], w_ref[at, 0:both], preferred_element_type=F32)
        acc_ref[...] = part if i == 0 else acc_ref[...] + part
    gate = acc_ref[:, 0:units]
    up = acc_ref[:, units:both]
    hidden = (gate / (1.0 + jnp.exp(-gate)) * up).astype(BF16)
    if spare:
        hidden = jnp.concatenate([hidden, jnp.zeros((hidden.shape[0], spare), BF16)], axis=1)
    nt = (((1,), (1,)), ((), ()))
    for i in range(depth // 256):
        at = pl.ds(i * 256, 256)
        o_ref[:, at] = lax.dot_general(
            hidden, w_ref[at, both:], nt, preferred_element_type=F32
        ).astype(BF16)


def feed(x, weights, units):
    rows, depth = x.shape
    width = weights.shape[1]
    pieces = 8
    return pl.pallas_call(
        functools.partial(feed_kernel, units=units),
        in_specs=[pl.BlockSpec(memory_space=pl.ANY)] * 2,
        out_specs=pl.BlockSpec(memory_space=pltpu.VMEM),
        out_shape=jax.ShapeDtypeStruct((rows, depth), BF16),
        scratch_shapes=[
            pltpu.VMEM((rows, depth), BF16),
            pltpu.VMEM((depth, width), BF16),
            pltpu.VMEM((rows, 2 * units), F32),
            pltpu.SemaphoreType.DMA((pieces + 1,)),
        ],
        compiler_params=pltpu.CompilerParams(vmem_limit_bytes=60 * 2**20),
        cost_estimate=pl.CostEstimate(
            flops=6 * rows * depth * units, bytes_accessed=10 * 2**20, transcendentals=0
        ),
        name="feed",
    )(x, weights)


def stream_kernel(part_ref, resid_ref, gain_ref, stream_ref, normed_ref):
    proj = part_ref[0].astype(F32)
    for n in range(1, part_ref.shape[0]):
        proj = proj + part_ref[n].astype(F32)
    stream = (resid_ref[...].astype(F32) + proj).astype(BF16)
    stream_ref[...] = stream
    values = stream.astype(F32)
    normed = values * lax.rsqrt(jnp.mean(values * values, axis=-1, keepdims=True) + EPSILON)
    normed_ref[...] = (normed * gain_ref[...]).astype(BF16)


def stream_rows(parts, resid, gain):
    return pl.pallas_call(
        stream_kernel,
        out_shape=(
            jax.ShapeDtypeStruct(resid.shape, BF16),
            jax.ShapeDtypeStruct(resid.shape, BF16),
        ),
        compiler_params=pltpu.CompilerParams(vmem_limit_bytes=8 * 2**20),
        cost_estimate=pl.CostEstimate(
            flops=8 * resid.size, bytes_accessed=2**20, transcendentals=0
        ),
        name="stream",
    )(parts, resid, gain.reshape(1, -1))


def scattered(x, axis):
    count = lax.axis_size(axis)
    return lax.all_to_all(x.reshape(count, -1, x.shape[1]), axis, 0, 0, tiled=True)


def body(
    resid,
    query,
    key,
    value,
    q_gain,
    k_gain,
    out_weight,
    norm_gain,
    gate_weight,
    up_weight,
    down_weight,
):
    rows = query.shape[0]
    units = gate_weight.shape[1]
    shard, copies, keys_values = prep(
        query,
        key,
        value,
        gate_weight,
        up_weight,
        down_weight.T,
        q_gain,
        k_gain,
        lax.axis_size("sp_0"),
    )
    weights = lax.all_gather(shard, SP, axis=0, tiled=True)
    queries = lax.all_to_all(copies, "sp_0", 0, 0, tiled=True)
    keys_values = lax.all_gather(keys_values, "sp_1", axis=0, tiled=True)
    other_weight = lax.ppermute(out_weight, "c", [(0, 1), (1, 0)])
    partial = lax.all_to_all(attend(queries, keys_values), "sp_0", 0, 0, tiled=True)
    attn = lax.all_gather(combine(partial), "c", axis=0)
    parts = scattered(project(attn, out_weight, other_weight), "x")
    share = rows // lax.axis_size(TP)
    my_resid = lax.dynamic_slice_in_dim(resid, lax.axis_index(TP) * share, share, 0)
    my_stream, normed = stream_rows(parts, my_resid, norm_gain)
    normed = lax.all_gather(normed, TP, axis=0, tiled=True)
    down = jnp.sum(scattered(feed(normed, weights, units), TP).astype(F32), axis=0)
    return (my_stream.astype(F32) + 0.5 * down).astype(BF16)


def solution(mesh):
    torus = Mesh(
        mesh.devices.reshape(8, 8, mesh.shape["tp"] // 2, 2), ("sp_0", "sp_1", "x", "c")
    )
    return jax.shard_map(
        body,
        mesh=torus,
        in_specs=(
            P(SP, None),
            P(SP, TP),
            P(SP, TP),
            P(SP, TP),
            P(),
            P(),
            P(TP, None),
            P(),
            P(SP, TP),
            P(SP, TP),
            P(TP, SP),
        ),
        out_specs=P(SP + TP, None),
        check_vma=False,
    )
```

```python
import functools

import jax
import jax.numpy as jnp
import numpy as np
from jax import lax
from jax.experimental import pallas as pl
from jax.experimental.pallas import tpu as pltpu
from jax.sharding import Mesh
from jax.sharding import PartitionSpec as P

GRID_W = 64
SP = ("sp_0", "sp_1")
TP = ("x", "c")
EPSILON = 1e-06
BF16 = jnp.bfloat16
F32 = jnp.float32
ROPE_BASE = 10000.0
STAT_ROWS = 16
LOG2E = 1.4426950408889634


def rope_tables(head_dim):
    quarter = head_dim // 4
    lane = np.arange(head_dim)
    inverse = np.power(np.float32(ROPE_BASE), -(lane % quarter).astype(np.float32) / np.float32(quarter))
    inverse = inverse.astype(np.float32)
    angles = np.arange(GRID_W, dtype=np.float32)[:, None] * inverse[None, :]
    sign = np.where((lane // quarter) % 2 == 0, -1.0, 1.0).astype(np.float32)
    cosine = np.cos(angles.astype(np.float64)).astype(np.float32)
    sine = np.sin(angles.astype(np.float64)).astype(np.float32) * sign
    return inverse[None, :], sign[None, :], cosine, sine


def prep_kernel(
    q_ref,
    k_ref,
    v_ref,
    gate_ref,
    up_ref,
    down_ref,
    qg_ref,
    kg_ref,
    inv_ref,
    sign_ref,
    cos_ref,
    sin_ref,
    wo_ref,
    qo_ref,
    kvo_ref,
):
    units = gate_ref.shape[1]
    for n, ref in enumerate((gate_ref, up_ref, down_ref)):
        wo_ref[:, n * units : (n + 1) * units] = ref[...]
    spare = wo_ref.shape[1] - 3 * units
    if spare:
        wo_ref[:, 3 * units :] = jnp.zeros((wo_ref.shape[0], spare), BF16)
    rows, head_dim = k_ref.shape
    heads = q_ref.shape[1] // head_dim
    quarter = head_dim // 4
    spans = rows // GRID_W
    sp = lax.axis_index("sp_0") * lax.axis_size("sp_1") + lax.axis_index("sp_1")
    first_row = (sp * spans).astype(F32)
    line = first_row + lax.broadcasted_iota(jnp.int32, (8, head_dim), 0).astype(F32)
    angle = line * inv_ref[...]
    row_cos = jnp.cos(angle)
    row_sin = jnp.sin(angle) * sign_ref[...]
    lane = lax.broadcasted_iota(jnp.int32, (GRID_W, head_dim), 1)
    by_row = lane < 2 * quarter
    is_first = (lane // quarter) % 2 == 0

    def turned(x, gain, cosine, sine):
        x = x.astype(F32)
        x = x * lax.rsqrt(jnp.mean(x * x, axis=-1, keepdims=True) + EPSILON) * gain
        other = jnp.where(
            is_first,
            pltpu.roll(x, head_dim - quarter, 1),
            pltpu.roll(x, quarter, 1),
        )
        return (x * cosine + other * sine).astype(BF16)

    for j in range(spans):
        at = pl.ds(j * GRID_W, GRID_W)
        cosine = jnp.where(by_row, row_cos[j : j + 1, :], cos_ref[...])
        sine = jnp.where(by_row, row_sin[j : j + 1, :], sin_ref[...])
        for h in range(heads):
            cols = slice(h * head_dim, (h + 1) * head_dim)
            made = turned(q_ref[at, cols], qg_ref[...], cosine, sine)
            for n in range(qo_ref.shape[0]):
                qo_ref[n, at, cols] = made
        kvo_ref[at, 0:head_dim] = turned(k_ref[at, :], kg_ref[...], cosine, sine)
    kvo_ref[:, head_dim:] = v_ref[...]


def prep(query, key, value, gate, up, down, q_gain, k_gain, copies):
    rows, head_dim = key.shape
    inverse, sign, cosine, sine = rope_tables(head_dim)
    return pl.pallas_call(
        prep_kernel,
        out_shape=(
            jax.ShapeDtypeStruct((gate.shape[0], -(-3 * gate.shape[1] // 128) * 128), BF16),
            jax.ShapeDtypeStruct((copies, *query.shape), BF16),
            jax.ShapeDtypeStruct((rows, 2 * head_dim), BF16),
        ),
        name="prep",
    )(
        query,
        key,
        value,
        gate,
        up,
        down,
        q_gain.reshape(1, -1),
        k_gain.reshape(1, -1),
        jnp.asarray(inverse),
        jnp.asarray(sign),
        jnp.asarray(cosine),
        jnp.asarray(sine),
    )


def split3(x):
    a = x.astype(BF16)
    rest = x - a.astype(F32)
    b = rest.astype(BF16)
    c = (rest - b.astype(F32)).astype(BF16)
    return a, b, c


def packed_stats(level):
    rows = level.shape[0]
    eye = (
        lax.broadcasted_iota(jnp.int32, (128, 128), 0)
        == lax.broadcasted_iota(jnp.int32, (128, 128), 1)
    )
    place = lax.broadcasted_iota(jnp.int32, (STAT_ROWS, 128), 0)
    out = jnp.zeros((STAT_ROWS, 128), F32)
    for t in range(-(-rows // 128)):
        n = min(128, rows - t * 128)
        spread = jnp.broadcast_to(level[t * 128 : t * 128 + n], (n, 128))
        flat = jnp.sum(jnp.where(eye[:n], spread, 0.0), axis=0, keepdims=True)
        for k, piece in enumerate(split3(flat)):
            out = jnp.where(place == 3 * t + k, piece.astype(F32), out)
    return out.astype(BF16)


def attend_kernel(q_ref, next_ref, kv_ref, o_ref, even_ref, odd_ref, top_ref, *, chunk):
    rows = q_ref.shape[1]
    head_dim = q_ref.shape[2] // 2
    count = kv_ref.shape[0] // chunk
    factor = head_dim ** (-0.5) * LOG2E

    def score(q, s_ref, c, peak):
        at = pl.ds(c * chunk, chunk)
        s = lax.dot_general(
            q, kv_ref[at, 0:head_dim], (((1,), (1,)), ((), ())), preferred_element_type=F32
        )
        s_ref[:, at] = s
        for u in range(chunk // 128):
            x = s[:, u * 128 : (u + 1) * 128]
            peak = x if peak is None else jnp.maximum(peak, x)
        return peak

    def weigh(s_ref, top, c, total, accum):
        at = pl.ds(c * chunk, chunk)
        w = jnp.exp2((s_ref[:, at] - top) * factor)
        for u in range(chunk // 128):
            x = w[:, u * 128 : (u + 1) * 128]
            total = x if total is None else total + x
        d = jnp.dot(w.astype(BF16), kv_ref[at, head_dim:], preferred_element_type=F32)
        return total, d if accum is None else accum + d

    def finish(b, top, total, accum):
        whole = jnp.sum(total, axis=-1, keepdims=True)
        cols = slice(b * head_dim, (b + 1) * head_dim)
        o_ref[0, 0:rows, cols] = (accum / whole).astype(BF16)
        o_ref[0, rows:, cols] = packed_stats(top * factor + jnp.log2(whole))

    @pl.when(pl.program_id(0) == 0)
    def _():
        peak = None
        for c in range(count):
            peak = score(q_ref[0, :, 0:head_dim], even_ref, c, peak)
        top_ref[...] = jnp.broadcast_to(jnp.max(peak, axis=-1, keepdims=True), top_ref.shape)

    top = top_ref[:, 0:1]
    for b, (q, s_ref, done_ref) in enumerate(
        ((q_ref[0, :, head_dim:], odd_ref, even_ref), (next_ref[0, :, 0:head_dim], even_ref, odd_ref))
    ):
        peak = total = accum = None
        for c in range(count):
            peak = score(q, s_ref, c, peak)
            total, accum = weigh(done_ref, top, c, total, accum)
        finish(b, top, total, accum)
        top = jnp.max(peak, axis=-1, keepdims=True)
    top_ref[...] = jnp.broadcast_to(top, top_ref.shape)


def attend(queries, keys_values):
    parts, rows, width = queries.shape
    keys = keys_values.shape[0]
    head_dim = width // 2
    work = parts * 2 * rows * keys
    return pl.pallas_call(
        functools.partial(
            attend_kernel, chunk=next(n for n in (512, 384, 256, 128) if keys % n == 0)
        ),
        grid=(parts,),
        in_specs=[
            pl.BlockSpec((1, rows, width), lambda i: (i, 0, 0)),
            pl.BlockSpec((1, rows, width), lambda i: (jnp.minimum(i + 1, parts - 1), 0, 0)),
            pl.BlockSpec((keys, 2 * head_dim), lambda i: (0, 0)),
        ],
        out_specs=pl.BlockSpec((1, rows + STAT_ROWS, width), lambda i: (i, 0, 0)),
        out_shape=jax.ShapeDtypeStruct((parts, rows + STAT_ROWS, width), BF16),
        scratch_shapes=[
            pltpu.VMEM((rows, keys), F32),
            pltpu.VMEM((rows, keys), F32),
            pltpu.VMEM((rows, 128), F32),
        ],
        compiler_params=pltpu.CompilerParams(
            dimension_semantics=("arbitrary",), vmem_limit_bytes=32 * 2**20
        ),
        cost_estimate=pl.CostEstimate(
            flops=4 * work * head_dim, bytes_accessed=4 * 2**20, transcendentals=work
        ),
        name="attend",
    )(queries, queries, keys_values)


def combine_kernel(part_ref, o_ref):
    parts, all_rows, width = part_ref.shape
    rows = all_rows - STAT_ROWS
    cores, held = o_ref.shape[:2]
    share = rows // lax.axis_size(TP)
    eye = (
        lax.broadcasted_iota(jnp.int32, (128, 128), 0)
        == lax.broadcasted_iota(jnp.int32, (128, 128), 1)
    )
    for h in range(width // 128):
        cols = slice(h * 128, (h + 1) * 128)
        stats = [part_ref[p, rows:, cols].astype(F32) for p in range(parts)]
        outs = []
        for t in range(-(-rows // 128)):
            n = min(128, rows - t * 128)
            levels = [
                s[3 * t : 3 * t + 1] + s[3 * t + 1 : 3 * t + 2] + s[3 * t + 2 : 3 * t + 3]
                for s in stats
            ]
            top = functools.reduce(jnp.maximum, levels)
            shares = [jnp.exp2(v - top) for v in levels]
            whole = functools.reduce(jnp.add, shares)
            total = jnp.zeros((n, 128), F32)
            for p in range(parts):
                flat = jnp.broadcast_to(shares[p] / whole, (n, 128))
                portion = jnp.sum(jnp.where(eye[:n], flat, 0.0), axis=1, keepdims=True)
                total = total + portion * part_ref[p, t * 128 : t * 128 + n, cols].astype(F32)
            outs.append(total)
        attn = jnp.concatenate(outs, axis=0)
        for k in range(rows // share):
            at = pl.ds(k // cores * share, share)
            o_ref[k % cores, at, cols] = attn[k * share : (k + 1) * share].astype(BF16)


def combine(parts):
    rows = parts.shape[1] - STAT_ROWS
    cores = lax.axis_size("c")
    return pl.pallas_call(
        combine_kernel,
        out_shape=jax.ShapeDtypeStruct((cores, rows // cores, parts.shape[2]), BF16),
        compiler_params=pltpu.CompilerParams(vmem_limit_bytes=16 * 2**20),
        cost_estimate=pl.CostEstimate(
            flops=2 * parts.size, bytes_accessed=2**20, transcendentals=0
        ),
        name="combine",
    )(parts)


def project_kernel(x_ref, own_ref, other_ref, o_ref):
    me = lax.axis_index("c")
    mine = x_ref[me, me]
    others = x_ref[1 - me, me]
    for c in range(own_ref.shape[1] // 512):
        at = pl.ds(c * 512, 512)
        o_ref[:, at] = (
            jnp.dot(mine, own_ref[:, at], preferred_element_type=F32)
            + jnp.dot(others, other_ref[:, at], preferred_element_type=F32)
        ).astype(BF16)


def project(attn, own, other):
    rows = attn.shape[2]
    return pl.pallas_call(
        project_kernel,
        out_shape=jax.ShapeDtypeStruct((rows, own.shape[1]), BF16),
        compiler_params=pltpu.CompilerParams(vmem_limit_bytes=16 * 2**20),
        cost_estimate=pl.CostEstimate(
            flops=4 * rows * own.size, bytes_accessed=3 * 2**20, transcendentals=0
        ),
        name="project",
    )(attn, own, other)


def feed_kernel(x_ref, w_hbm, o_ref, w_ref, acc_ref, sems, *, units):
    depth, width = w_ref.shape
    pieces = sems.shape[0]
    block = depth // pieces
    both = 2 * units
    spare = width - 3 * units
    copies = []
    for i in range(pieces):
        at = pl.ds(i * block, block)
        copies.append(pltpu.make_async_copy(w_hbm.at[at], w_ref.at[at], sems.at[i]))
        copies[-1].start()
    for i in range(pieces):
        at = pl.ds(i * block, block)
        copies[i].wait()
        part = jnp.dot(x_ref[:, at], w_ref[at, 0:both], preferred_element_type=F32)
        acc_ref[...] = part if i == 0 else acc_ref[...] + part
    gate = acc_ref[:, 0:units]
    up = acc_ref[:, units:both]
    hidden = (gate / (1.0 + jnp.exp(-gate)) * up).astype(BF16)
    if spare:
        hidden = jnp.concatenate([hidden, jnp.zeros((hidden.shape[0], spare), BF16)], axis=1)
    nt = (((1,), (1,)), ((), ()))
    for i in range(depth // 256):
        at = pl.ds(i * 256, 256)
        o_ref[:, at] = lax.dot_general(
            hidden, w_ref[at, both:], nt, preferred_element_type=F32
        ).astype(BF16)


def feed(x, weights, units):
    rows, depth = x.shape
    width = weights.shape[1]
    pieces = 8
    vmem = pl.BlockSpec(memory_space=pltpu.VMEM)
    return pl.pallas_call(
        functools.partial(feed_kernel, units=units),
        in_specs=[vmem, pl.BlockSpec(memory_space=pl.ANY)],
        out_specs=vmem,
        out_shape=jax.ShapeDtypeStruct((rows, depth), BF16),
        scratch_shapes=[
            pltpu.VMEM((depth, width), BF16),
            pltpu.VMEM((rows, 2 * units), F32),
            pltpu.SemaphoreType.DMA((pieces,)),
        ],
        compiler_params=pltpu.CompilerParams(vmem_limit_bytes=50 * 2**20),
        cost_estimate=pl.CostEstimate(
            flops=6 * rows * depth * units, bytes_accessed=10 * 2**20, transcendentals=0
        ),
        name="feed",
    )(x, weights)


def stream_kernel(part_ref, resid_ref, gain_ref, stream_ref, normed_ref):
    proj = part_ref[0].astype(F32)
    for n in range(1, part_ref.shape[0]):
        proj = proj + part_ref[n].astype(F32)
    stream = (resid_ref[...].astype(F32) + proj).astype(BF16)
    stream_ref[...] = stream
    values = stream.astype(F32)
    normed = values * lax.rsqrt(jnp.mean(values * values, axis=-1, keepdims=True) + EPSILON)
    normed_ref[...] = (normed * gain_ref[...]).astype(BF16)


def stream_rows(parts, resid, gain):
    return pl.pallas_call(
        stream_kernel,
        out_shape=(
            jax.ShapeDtypeStruct(resid.shape, BF16),
            jax.ShapeDtypeStruct(resid.shape, BF16),
        ),
        compiler_params=pltpu.CompilerParams(vmem_limit_bytes=8 * 2**20),
        cost_estimate=pl.CostEstimate(
            flops=8 * resid.size, bytes_accessed=2**20, transcendentals=0
        ),
        name="stream",
    )(parts, resid, gain.reshape(1, -1))


def scattered(x, axis):
    count = lax.axis_size(axis)
    return lax.all_to_all(x.reshape(count, -1, x.shape[1]), axis, 0, 0, tiled=True)


def body(
    resid,
    query,
    key,
    value,
    q_gain,
    k_gain,
    out_weight,
    norm_gain,
    gate_weight,
    up_weight,
    down_weight,
):
    rows = query.shape[0]
    units = gate_weight.shape[1]
    shard, copies, keys_values = prep(
        query,
        key,
        value,
        gate_weight,
        up_weight,
        down_weight.T,
        q_gain,
        k_gain,
        lax.axis_size("sp_0"),
    )
    weights = lax.all_gather(shard, SP, axis=0, tiled=True)
    queries = lax.all_to_all(copies, "sp_0", 0, 0, tiled=True)
    keys_values = lax.all_gather(keys_values, "sp_1", axis=0, tiled=True)
    other_weight = lax.ppermute(out_weight, "c", [(0, 1), (1, 0)])
    partial = lax.all_to_all(attend(queries, keys_values), "sp_0", 0, 0, tiled=True)
    attn = lax.all_gather(combine(partial), "c", axis=0)
    parts = scattered(project(attn, out_weight, other_weight), "x")
    share = rows // lax.axis_size(TP)
    my_resid = lax.dynamic_slice_in_dim(resid, lax.axis_index(TP) * share, share, 0)
    my_stream, normed = stream_rows(parts, my_resid, norm_gain)
    normed = lax.all_gather(normed, TP, axis=0, tiled=True)
    down = jnp.sum(scattered(feed(normed, weights, units), TP).astype(F32), axis=0)
    return (my_stream.astype(F32) + 0.5 * down).astype(BF16)


def solution(mesh):
    torus = Mesh(
        mesh.devices.reshape(8, 8, mesh.shape["tp"] // 2, 2), ("sp_0", "sp_1", "x", "c")
    )
    return jax.shard_map(
        body,
        mesh=torus,
        in_specs=(
            P(SP, None),
            P(SP, TP),
            P(SP, TP),
            P(SP, TP),
            P(),
            P(),
            P(TP, None),
            P(),
            P(SP, TP),
            P(SP, TP),
            P(TP, SP),
        ),
        out_specs=P(SP + TP, None),
        check_vma=False,
    )
```

```python
import functools

import jax
import jax.numpy as jnp
import numpy as np
from jax import lax
from jax.experimental import pallas as pl
from jax.experimental.pallas import tpu as pltpu
from jax.sharding import Mesh
from jax.sharding import PartitionSpec as P

GRID_W = 64
SP = ("sp_0", "sp_1")
TP = ("x", "c")
EPSILON = 1e-06
BF16 = jnp.bfloat16
F32 = jnp.float32
ROPE_BASE = 10000.0
STAT_ROWS = 8
LOG2E = 1.4426950408889634


def rope_tables(head_dim):
    quarter = head_dim // 4
    lane = np.arange(head_dim)
    inverse = np.power(np.float32(ROPE_BASE), -(lane % quarter).astype(np.float32) / np.float32(quarter))
    inverse = inverse.astype(np.float32)
    angles = np.arange(GRID_W, dtype=np.float32)[:, None] * inverse[None, :]
    sign = np.where((lane // quarter) % 2 == 0, -1.0, 1.0).astype(np.float32)
    cosine = np.cos(angles.astype(np.float64)).astype(np.float32)
    sine = np.sin(angles.astype(np.float64)).astype(np.float32) * sign
    return inverse[None, :], sign[None, :], cosine, sine


def prep_kernel(
    q_ref,
    k_ref,
    v_ref,
    gate_ref,
    up_ref,
    down_ref,
    qg_ref,
    kg_ref,
    inv_ref,
    sign_ref,
    cos_ref,
    sin_ref,
    wo_ref,
    qo_ref,
    kvo_ref,
):
    units = gate_ref.shape[1]
    for n, ref in enumerate((gate_ref, up_ref, down_ref)):
        wo_ref[:, n * units : (n + 1) * units] = ref[...]
    spare = wo_ref.shape[1] - 3 * units
    if spare:
        wo_ref[:, 3 * units :] = jnp.zeros((wo_ref.shape[0], spare), BF16)
    rows, head_dim = k_ref.shape
    heads = q_ref.shape[1] // head_dim
    quarter = head_dim // 4
    spans = rows // GRID_W
    sp = lax.axis_index("sp_0") * lax.axis_size("sp_1") + lax.axis_index("sp_1")
    first_row = (sp * spans).astype(F32)
    line = first_row + lax.broadcasted_iota(jnp.int32, (8, head_dim), 0).astype(F32)
    angle = line * inv_ref[...]
    row_cos = jnp.cos(angle)
    row_sin = jnp.sin(angle) * sign_ref[...]
    lane = lax.broadcasted_iota(jnp.int32, (GRID_W, head_dim), 1)
    by_row = lane < 2 * quarter
    is_first = (lane // quarter) % 2 == 0

    def turned(x, gain, cosine, sine):
        x = x.astype(F32)
        x = x * lax.rsqrt(jnp.mean(x * x, axis=-1, keepdims=True) + EPSILON) * gain
        other = jnp.where(
            is_first,
            pltpu.roll(x, head_dim - quarter, 1),
            pltpu.roll(x, quarter, 1),
        )
        return (x * cosine + other * sine).astype(BF16)

    for j in range(spans):
        at = pl.ds(j * GRID_W, GRID_W)
        cosine = jnp.where(by_row, row_cos[j : j + 1, :], cos_ref[...])
        sine = jnp.where(by_row, row_sin[j : j + 1, :], sin_ref[...])
        for h in range(heads):
            cols = slice(h * head_dim, (h + 1) * head_dim)
            made = turned(q_ref[at, cols], qg_ref[...], cosine, sine)
            for n in range(qo_ref.shape[0]):
                qo_ref[n, at, cols] = made
        kvo_ref[at, 0:head_dim] = turned(k_ref[at, :], kg_ref[...], cosine, sine)
    kvo_ref[:, head_dim:] = v_ref[...]


def prep(query, key, value, gate, up, down, q_gain, k_gain, copies):
    rows, head_dim = key.shape
    inverse, sign, cosine, sine = rope_tables(head_dim)
    return pl.pallas_call(
        prep_kernel,
        out_shape=(
            jax.ShapeDtypeStruct((gate.shape[0], -(-3 * gate.shape[1] // 128) * 128), BF16),
            jax.ShapeDtypeStruct((copies, *query.shape), BF16),
            jax.ShapeDtypeStruct((rows, 2 * head_dim), BF16),
        ),
        name="prep",
    )(
        query,
        key,
        value,
        gate,
        up,
        down,
        q_gain.reshape(1, -1),
        k_gain.reshape(1, -1),
        jnp.asarray(inverse),
        jnp.asarray(sign),
        jnp.asarray(cosine),
        jnp.asarray(sine),
    )


def split3(x):
    a = x.astype(BF16)
    rest = x - a.astype(F32)
    b = rest.astype(BF16)
    c = (rest - b.astype(F32)).astype(BF16)
    return a, b, c


def packed_stats(level):
    rows = level.shape[0]
    eye = (
        lax.broadcasted_iota(jnp.int32, (128, 128), 0)
        == lax.broadcasted_iota(jnp.int32, (128, 128), 1)
    )
    place = lax.broadcasted_iota(jnp.int32, (STAT_ROWS, 128), 0)
    out = jnp.zeros((STAT_ROWS, 128), F32)
    for t in range(-(-rows // 128)):
        n = min(128, rows - t * 128)
        spread = jnp.broadcast_to(level[t * 128 : t * 128 + n], (n, 128))
        flat = jnp.sum(jnp.where(eye[:n], spread, 0.0), axis=0, keepdims=True)
        for k, piece in enumerate(split3(flat)):
            out = jnp.where(place == 3 * t + k, piece.astype(F32), out)
    return out.astype(BF16)


def attend_kernel(q_ref, next_ref, kv_ref, o_ref, even_ref, odd_ref, top_ref, *, chunk):
    rows = q_ref.shape[1]
    head_dim = q_ref.shape[2] // 2
    count = kv_ref.shape[0] // chunk
    factor = head_dim ** (-0.5) * LOG2E

    def score(q, s_ref, c, peak):
        at = pl.ds(c * chunk, chunk)
        s = lax.dot_general(
            q, kv_ref[at, 0:head_dim], (((1,), (1,)), ((), ())), preferred_element_type=F32
        )
        s_ref[:, at] = s
        for u in range(chunk // 128):
            x = s[:, u * 128 : (u + 1) * 128]
            peak = x if peak is None else jnp.maximum(peak, x)
        return peak

    def weigh(s_ref, top, c, total, accum):
        at = pl.ds(c * chunk, chunk)
        w = jnp.exp2((s_ref[:, at] - top) * factor)
        for u in range(chunk // 128):
            x = w[:, u * 128 : (u + 1) * 128]
            total = x if total is None else total + x
        d = jnp.dot(w.astype(BF16), kv_ref[at, head_dim:], preferred_element_type=F32)
        return total, d if accum is None else accum + d

    def finish(b, top, total, accum):
        whole = jnp.sum(total, axis=-1, keepdims=True)
        cols = slice(b * head_dim, (b + 1) * head_dim)
        o_ref[0, 0:rows, cols] = (accum / whole).astype(BF16)
        o_ref[0, rows:, cols] = packed_stats(top * factor + jnp.log2(whole))

    @pl.when(pl.program_id(0) == 0)
    def _():
        peak = None
        for c in range(count):
            peak = score(q_ref[0, :, 0:head_dim], even_ref, c, peak)
        top_ref[...] = jnp.broadcast_to(jnp.max(peak, axis=-1, keepdims=True), top_ref.shape)

    top = top_ref[:, 0:1]
    for b, (q, s_ref, done_ref) in enumerate(
        ((q_ref[0, :, head_dim:], odd_ref, even_ref), (next_ref[0, :, 0:head_dim], even_ref, odd_ref))
    ):
        peak = total = accum = None
        for c in range(count):
            peak = score(q, s_ref, c, peak)
            total, accum = weigh(done_ref, top, c, total, accum)
        finish(b, top, total, accum)
        top = jnp.max(peak, axis=-1, keepdims=True)
    top_ref[...] = jnp.broadcast_to(top, top_ref.shape)


def attend(queries, keys_values):
    parts, rows, width = queries.shape
    keys = keys_values.shape[0]
    head_dim = width // 2
    work = parts * 2 * rows * keys
    return pl.pallas_call(
        functools.partial(
            attend_kernel, chunk=next(n for n in (512, 384, 256, 128) if keys % n == 0)
        ),
        grid=(parts,),
        in_specs=[
            pl.BlockSpec((1, rows, width), lambda i: (i, 0, 0)),
            pl.BlockSpec((1, rows, width), lambda i: (jnp.minimum(i + 1, parts - 1), 0, 0)),
            pl.BlockSpec((keys, 2 * head_dim), lambda i: (0, 0)),
        ],
        out_specs=pl.BlockSpec((1, rows + STAT_ROWS, width), lambda i: (i, 0, 0)),
        out_shape=jax.ShapeDtypeStruct((parts, rows + STAT_ROWS, width), BF16),
        scratch_shapes=[
            pltpu.VMEM((rows, keys), F32),
            pltpu.VMEM((rows, keys), F32),
            pltpu.VMEM((rows, 128), F32),
        ],
        compiler_params=pltpu.CompilerParams(
            dimension_semantics=("arbitrary",), vmem_limit_bytes=32 * 2**20
        ),
        cost_estimate=pl.CostEstimate(
            flops=4 * work * head_dim, bytes_accessed=4 * 2**20, transcendentals=work
        ),
        name="attend",
    )(queries, queries, keys_values)


def combine_kernel(part_ref, o_ref):
    parts, all_rows, width = part_ref.shape
    rows = all_rows - STAT_ROWS
    cores, held = o_ref.shape[:2]
    share = rows // lax.axis_size(TP)
    eye = (
        lax.broadcasted_iota(jnp.int32, (128, 128), 0)
        == lax.broadcasted_iota(jnp.int32, (128, 128), 1)
    )
    for h in range(width // 128):
        cols = slice(h * 128, (h + 1) * 128)
        stats = [part_ref[p, rows:, cols].astype(F32) for p in range(parts)]
        outs = []
        for t in range(-(-rows // 128)):
            n = min(128, rows - t * 128)
            levels = [
                s[3 * t : 3 * t + 1] + s[3 * t + 1 : 3 * t + 2] + s[3 * t + 2 : 3 * t + 3]
                for s in stats
            ]
            top = functools.reduce(jnp.maximum, levels)
            shares = [jnp.exp2(v - top) for v in levels]
            whole = functools.reduce(jnp.add, shares)
            total = jnp.zeros((n, 128), F32)
            for p in range(parts):
                flat = jnp.broadcast_to(shares[p] / whole, (n, 128))
                portion = jnp.sum(jnp.where(eye[:n], flat, 0.0), axis=1, keepdims=True)
                total = total + portion * part_ref[p, t * 128 : t * 128 + n, cols].astype(F32)
            outs.append(total)
        attn = jnp.concatenate(outs, axis=0)
        for k in range(rows // share):
            at = pl.ds(k // cores * share, share)
            o_ref[k % cores, at, cols] = attn[k * share : (k + 1) * share].astype(BF16)


def combine(parts):
    rows = parts.shape[1] - STAT_ROWS
    cores = lax.axis_size("c")
    return pl.pallas_call(
        combine_kernel,
        out_shape=jax.ShapeDtypeStruct((cores, rows // cores, parts.shape[2]), BF16),
        compiler_params=pltpu.CompilerParams(vmem_limit_bytes=16 * 2**20),
        cost_estimate=pl.CostEstimate(
            flops=2 * parts.size, bytes_accessed=2**20, transcendentals=0
        ),
        name="combine",
    )(parts)


def project_kernel(x_ref, own_ref, other_ref, o_ref):
    me = lax.axis_index("c")
    mine = x_ref[me, me]
    others = x_ref[1 - me, me]
    for c in range(own_ref.shape[1] // 512):
        at = pl.ds(c * 512, 512)
        o_ref[:, at] = (
            jnp.dot(mine, own_ref[:, at], preferred_element_type=F32)
            + jnp.dot(others, other_ref[:, at], preferred_element_type=F32)
        ).astype(BF16)


def project(attn, own, other):
    rows = attn.shape[2]
    return pl.pallas_call(
        project_kernel,
        out_shape=jax.ShapeDtypeStruct((rows, own.shape[1]), BF16),
        compiler_params=pltpu.CompilerParams(vmem_limit_bytes=16 * 2**20),
        cost_estimate=pl.CostEstimate(
            flops=4 * rows * own.size, bytes_accessed=3 * 2**20, transcendentals=0
        ),
        name="project",
    )(attn, own, other)


def feed_kernel(x_ref, w_hbm, o_ref, w_ref, acc_ref, sems, *, units):
    depth, width = w_ref.shape
    pieces = sems.shape[0]
    block = depth // pieces
    both = 2 * units
    spare = width - 3 * units
    copies = []
    for i in range(pieces):
        at = pl.ds(i * block, block)
        copies.append(pltpu.make_async_copy(w_hbm.at[at], w_ref.at[at], sems.at[i]))
        copies[-1].start()
    for i in range(pieces):
        at = pl.ds(i * block, block)
        copies[i].wait()
        part = jnp.dot(x_ref[:, at], w_ref[at, 0:both], preferred_element_type=F32)
        acc_ref[...] = part if i == 0 else acc_ref[...] + part
    gate = acc_ref[:, 0:units]
    up = acc_ref[:, units:both]
    hidden = (gate / (1.0 + jnp.exp(-gate)) * up).astype(BF16)
    if spare:
        hidden = jnp.concatenate([hidden, jnp.zeros((hidden.shape[0], spare), BF16)], axis=1)
    nt = (((1,), (1,)), ((), ()))
    for i in range(depth // 256):
        at = pl.ds(i * 256, 256)
        o_ref[:, at] = lax.dot_general(
            hidden, w_ref[at, both:], nt, preferred_element_type=F32
        ).astype(BF16)


def feed(x, weights, units):
    rows, depth = x.shape
    width = weights.shape[1]
    pieces = 8
    vmem = pl.BlockSpec(memory_space=pltpu.VMEM)
    return pl.pallas_call(
        functools.partial(feed_kernel, units=units),
        in_specs=[vmem, pl.BlockSpec(memory_space=pl.ANY)],
        out_specs=vmem,
        out_shape=jax.ShapeDtypeStruct((rows, depth), BF16),
        scratch_shapes=[
            pltpu.VMEM((depth, width), BF16),
            pltpu.VMEM((rows, 2 * units), F32),
            pltpu.SemaphoreType.DMA((pieces,)),
        ],
        compiler_params=pltpu.CompilerParams(vmem_limit_bytes=50 * 2**20),
        cost_estimate=pl.CostEstimate(
            flops=6 * rows * depth * units, bytes_accessed=10 * 2**20, transcendentals=0
        ),
        name="feed",
    )(x, weights)


def stream_kernel(part_ref, resid_ref, gain_ref, stream_ref, normed_ref):
    proj = part_ref[0].astype(F32)
    for n in range(1, part_ref.shape[0]):
        proj = proj + part_ref[n].astype(F32)
    stream = (resid_ref[...].astype(F32) + proj).astype(BF16)
    stream_ref[...] = stream
    values = stream.astype(F32)
    normed = values * lax.rsqrt(jnp.mean(values * values, axis=-1, keepdims=True) + EPSILON)
    normed_ref[...] = (normed * gain_ref[...]).astype(BF16)


def stream_rows(parts, resid, gain):
    return pl.pallas_call(
        stream_kernel,
        out_shape=(
            jax.ShapeDtypeStruct(resid.shape, BF16),
            jax.ShapeDtypeStruct(resid.shape, BF16),
        ),
        compiler_params=pltpu.CompilerParams(vmem_limit_bytes=8 * 2**20),
        cost_estimate=pl.CostEstimate(
            flops=8 * resid.size, bytes_accessed=2**20, transcendentals=0
        ),
        name="stream",
    )(parts, resid, gain.reshape(1, -1))


def scattered(x, axis):
    count = lax.axis_size(axis)
    return lax.all_to_all(x.reshape(count, -1, x.shape[1]), axis, 0, 0, tiled=True)


def body(
    resid,
    query,
    key,
    value,
    q_gain,
    k_gain,
    out_weight,
    norm_gain,
    gate_weight,
    up_weight,
    down_weight,
):
    rows = query.shape[0]
    units = gate_weight.shape[1]
    shard, copies, keys_values = prep(
        query,
        key,
        value,
        gate_weight,
        up_weight,
        down_weight.T,
        q_gain,
        k_gain,
        lax.axis_size("sp_0"),
    )
    weights = lax.all_gather(shard, SP, axis=0, tiled=True)
    queries = lax.all_to_all(copies, "sp_0", 0, 0, tiled=True)
    keys_values = lax.all_gather(keys_values, "sp_1", axis=0, tiled=True)
    other_weight = lax.ppermute(out_weight, "c", [(0, 1), (1, 0)])
    partial = lax.all_to_all(attend(queries, keys_values), "sp_0", 0, 0, tiled=True)
    attn = lax.all_gather(combine(partial), "c", axis=0)
    parts = scattered(project(attn, out_weight, other_weight), "x")
    share = rows // lax.axis_size(TP)
    my_resid = lax.dynamic_slice_in_dim(resid, lax.axis_index(TP) * share, share, 0)
    my_stream, normed = stream_rows(parts, my_resid, norm_gain)
    normed = lax.all_gather(normed, TP, axis=0, tiled=True)
    down = jnp.sum(scattered(feed(normed, weights, units), TP).astype(F32), axis=0)
    return (my_stream.astype(F32) + 0.5 * down).astype(BF16)


def solution(mesh):
    torus = Mesh(
        mesh.devices.reshape(8, 8, mesh.shape["tp"] // 2, 2), ("sp_0", "sp_1", "x", "c")
    )
    return jax.shard_map(
        body,
        mesh=torus,
        in_specs=(
            P(SP, None),
            P(SP, TP),
            P(SP, TP),
            P(SP, TP),
            P(),
            P(),
            P(TP, None),
            P(),
            P(SP, TP),
            P(SP, TP),
            P(TP, SP),
        ),
        out_specs=P(SP + TP, None),
        check_vma=False,
    )
```
